32 devices in a mesh: ep: 4 (over y, x), tp: 8 (over z, core).
Axes of the slice: x: 2, y: 2, z: 4, core: 2. Of those that a mesh axis runs over, the one named last changes fastest.
Arguments:
- query_latent: bfloat16 [2048, 1024], P('ep'), may hold values from -6 to 6
- joint_latent: bfloat16 [2048, 512], P('ep'), may hold values from -6 to 6
- rotary_key: bfloat16 [2048, 32], P('ep'), may hold values from -60 to 60
- query_gain: float32 [1024], replicated, may hold values from 0.1 to 1.9
- joint_gain: float32 [512], replicated, may hold values from 0.1 to 1.9
- query_weight: bfloat16 [1024, 2048], P(None, 'tp'), may hold values from -0.1875 to 0.1875
- query_rotary: bfloat16 [1024, 1024], P(None, 'tp'), may hold values from -0.1875 to 0.1875
- key_weight: bfloat16 [512, 2048], P(None, 'tp'), may hold values from -0.25 to 0.25
- value_weight: bfloat16 [512, 2048], P(None, 'tp'), may hold values from -0.25 to 0.25
- output_weight: bfloat16 [2048, 2048], P('tp'), may hold values from -6 to 6
- expert_input: bfloat16 [2048, 2048], P('ep'), may hold values from -6 to 6
- expert_gain: float32 [2048], replicated, may hold values from 0.1 to 1.9
- routes: int32 [2048, 2], P('ep'), may hold values from 0 to 7, all different within a row; in each aligned block of 512 rows (0 to 511, 512 to 1023, ...) at most 192 rows name the same one
- route_weight: float32 [2048, 2], P('ep'), may hold values from 0.2 to 1
- gate_weight: bfloat16 [8, 2048, 4096], P('ep', None, 'tp'), may hold values from -0.125 to 0.125
- up_weight: bfloat16 [8, 2048, 4096], P('ep', None, 'tp'), may hold values from -0.125 to 0.125
- down_weight: bfloat16 [8, 4096, 2048], P('ep', 'tp'), may hold values from -0.09375 to 0.09375
Outputs:
- mixer_out: bfloat16 [2048, 2048], P(('ep', 'tp'))
- expert_out: bfloat16 [2048, 2048], P('ep', 'tp')
The draws below stay inside these ranges and needn't reach their ends.
Inputs may be any that keep to these rules, and one draw needn't show every extreme that they name: `routes`: A row names 2 different experts. Among the rows of one device (aligned blocks of 512 rows) no expert is named by more than 192 rows, a bound that some block reaches.
All inputs are finite; a program needn't handle non-finite values.
Results may differ from the reference program's by a relative error of at most 0.019.
The reference program's roundings to bfloat16 on the way count: a program that leaves them out, or rounds other values in their place, can miss the bound.
Values may be sent and summed in bfloat16 or wider, within the bound.
A program may use at most 128 MiB of HBM per device.

```python
import math
import jax
import jax.numpy as jnp
import numpy as np
from jax import lax

D = 2048
HEADS = 32
NOPE = 64
ROPE = 32
VDIM = 64
QL = 1024
KVL = 512
FF = 4096
TOPK = 2
TOK_B_DEV = 512
EXPERTS = 8
TOK_A = 2048
TOK_B = 2048
CAP = 192
N_EP = 4
N_TP = 8


def draw_rotary_key(key, part):
    base = jax.random.normal(jax.random.fold_in(key, 11), (TOK_A, ROPE), jnp.float32)
    return jnp.clip(base, -60.0, 60.0).astype(jnp.bfloat16)


def level_of(stream_key, shape, shards, low, high):
    def one(dim, blocks):
        draws = jax.random.uniform(jax.random.fold_in(jax.random.fold_in(stream_key, 6), dim), (blocks,), jnp.float32, low / len(shards), high / len(shards))
        return jnp.repeat(jnp.exp(draws), shape[dim] // blocks).reshape((-1,) + (1,) * (len(shape) - dim - 1))

    gain = one(*shards[0])
    for cut in shards[1:]:
        gain = gain * one(*cut)
    return gain


def deal_out(rng, own, number, rows, amount, top, most, slope):
    sequence = jax.random.permutation(rng, amount)
    packed, usual = load_shares(amount, rows * top, most, slope, True), load_shares(amount, rows * top, most, slope, False)
    places = jnp.arange(amount)

    def named(sizes, rotation):
        used = int((sizes > 0).sum())
        fixed = max(1, used // 4)
        passed = fixed + (places - fixed + rotation * (used - fixed)) % max(1, amount - fixed)
        return jnp.zeros((amount,), jnp.int32).at[sequence[jnp.where(places < fixed, places, passed)]].set(jnp.asarray(sizes, jnp.int32))

    sizes = jnp.where(number % 4 == 0, named(packed, number // 4), named(usual, number - number // 4 - 1))
    mixed = jax.random.permutation(jax.random.fold_in(own, 3), amount)
    giver, receiver = mixed[0:amount // 2 * 2:2], mixed[1:amount // 2 * 2:2]
    margin = jnp.minimum(sizes[giver] - 1, most - sizes[receiver]) // 2
    margin = jnp.where((giver == sequence[0]) | (receiver == sequence[0]) | (sizes[receiver] == 0), 0, jnp.maximum(margin, 0))
    passed = jax.random.randint(jax.random.fold_in(own, 4), (amount // 2,), 0, 1 << 20) % (margin + 1)
    sizes = sizes.at[giver].add(-passed).at[receiver].add(passed)
    members = jnp.searchsorted(jnp.cumsum(sizes), jnp.arange(rows * top), side="right").astype(jnp.int32)
    listing = members.reshape(top, rows).T
    listing = listing[jax.random.permutation(jax.random.fold_in(own, 1), rows)]
    rotation = jax.random.randint(jax.random.fold_in(own, 2), (rows, 1), 0, top)
    return jnp.take_along_axis(listing, (jnp.arange(top)[None, :] + rotation) % top, axis=1)


def load_shares(count, total, reach, skew, full):
    weights = [(1 << 20) // math.isqrt(grade ** skew) + 1 for grade in range(1, count + 1)]
    largest = reach if full else min(reach, max(-(-total // count), total * weights[0] // sum(weights)))
    least = 1 if total - largest >= count - 1 else 0
    given, rest = [largest] + [least] * (count - 1), total - largest - least * (count - 1)
    while rest > 0:
        free = [i for i in range(1, count) if given[i] < largest] or [i for i in range(1, count) if given[i] < reach]
        mass, remaining = sum([weights[i] for i in free]), rest
        for i in free:
            addition = min(reach - given[i], max(1, remaining * weights[i] // mass), rest)
            given[i] = given[i] + addition
            rest = rest - addition
    return np.array(given)


def gaussian(stream_key, dims, scale, bound, cuts=(), kind=jnp.bfloat16):
    loudness = level_of(stream_key, dims, cuts, -0.22, 0.18) if cuts else 1.0
    result = jax.random.normal(stream_key, dims, jnp.float32) * scale * loudness
    return jnp.minimum(jnp.maximum(result, -bound), bound).astype(kind)


def setup_inputs(seed: int = 0) -> dict:
    keys = jax.random.split(jax.random.key(seed), 18)
    query_latent = gaussian(keys[0], (TOK_A, QL), 1.0, 6.0, ((0, 4),))
    joint_latent = gaussian(keys[1], (TOK_A, KVL), 1.0, 6.0, ((0, 4),))
    rotary_key = draw_rotary_key(jax.random.fold_in(keys[17], 71), 0)
    query_gain = jnp.clip(1.0 + 0.18 * jax.random.normal(keys[3], (QL,), jnp.float32), 0.1, 1.9)
    joint_gain = jnp.clip(1.0 + 0.18 * jax.random.normal(keys[4], (KVL,), jnp.float32), 0.1, 1.9)
    query_weight = gaussian(keys[5], (QL, HEADS * NOPE), QL ** -0.5, 0.1875, ((1, 8),))
    query_rotary = gaussian(keys[6], (QL, HEADS * ROPE), QL ** -0.5, 0.1875, ((1, 8),))
    key_weight = gaussian(keys[7], (KVL, HEADS * NOPE), KVL ** -0.5, 0.25, ((1, 8),))
    value_weight = gaussian(keys[8], (KVL, HEADS * VDIM), KVL ** -0.5, 0.25, ((1, 8),))
    output_weight = gaussian(keys[9], (HEADS * VDIM, D), 1.0, 6.0, ((0, 8),))
    expert_input = gaussian(keys[10], (TOK_B, D), 1.0, 6.0, ((0, 4),))
    expert_gain = jnp.clip(1.0 + 0.18 * jax.random.normal(keys[11], (D,), jnp.float32), 0.1, 1.9)
    routes_keys = jax.random.split(jax.random.fold_in(keys[12], 1), TOK_B // TOK_B_DEV)
    routes_turns = jax.random.permutation(jax.random.fold_in(keys[12], 3), TOK_B // TOK_B_DEV)
    routes = jax.vmap(lambda own, number: deal_out(jax.random.fold_in(keys[12], 2), own, number, TOK_B_DEV, EXPERTS, TOPK, CAP, 1))(routes_keys, routes_turns).reshape((TOK_B, TOPK))
    route_weight = jnp.clip(0.2 + 0.8 * jax.random.uniform(keys[13], (TOK_B, TOPK), jnp.float32) ** level_of(keys[13], (TOK_B, TOPK), ((0, 4),), -0.2, 0.2), 0.2, 1.0)
    gate_weight = gaussian(keys[14], (EXPERTS, D, FF), D ** -0.5, 0.125, ((0, 4), (2, 8)))
    up_weight = gaussian(keys[15], (EXPERTS, D, FF), D ** -0.5, 0.125, ((0, 4), (2, 8)))
    down_weight = gaussian(keys[16], (EXPERTS, FF, D), FF ** -0.5, 0.09375, ((0, 4), (1, 8)))
    return dict(query_latent=query_latent, joint_latent=joint_latent, rotary_key=rotary_key, query_gain=query_gain, joint_gain=joint_gain, query_weight=query_weight, query_rotary=query_rotary, key_weight=key_weight, value_weight=value_weight, output_weight=output_weight, expert_input=expert_input, expert_gain=expert_gain, routes=routes, route_weight=route_weight, gate_weight=gate_weight, up_weight=up_weight, down_weight=down_weight)


NORM_EPSILON = 1e-06
ROTARY_BASE = 10000.0

def norm_rows(source, gain_vector):
    as_float = source.astype(jnp.float32)
    factor = lax.rsqrt(lax.optimization_barrier(jnp.mean(as_float * as_float, axis=-1, keepdims=True)) + NORM_EPSILON)
    return (as_float * factor * gain_vector.astype(jnp.float32)).astype(jnp.bfloat16)

def rotate(source, positions):
    half_width = source.shape[-1] // 2
    frequencies = ROTARY_BASE ** (-jnp.arange(half_width, dtype=jnp.float32) / half_width)
    angles = positions[:, None] * frequencies[None, :]
    view_shape = (source.shape[0],) + (1,) * (source.ndim - 2) + (half_width,)
    cosine_table = jnp.cos(angles).reshape(view_shape)
    sine_table = jnp.sin(angles).reshape(view_shape)
    first_half = source[..., :half_width]
    second = source[..., half_width:]
    return jnp.concatenate([first_half * cosine_table - second * sine_table, second * cosine_table + first_half * sine_table], axis=-1)

def reference(query_latent, joint_latent, rotary_key, query_gain, joint_gain, query_weight, query_rotary, key_weight, value_weight, output_weight, expert_input, expert_gain, routes, route_weight, gate_weight, up_weight, down_weight):
    positions = jnp.arange(TOK_A, dtype=jnp.float32)
    query_normed = norm_rows(query_latent, query_gain)
    joint_normed = norm_rows(joint_latent, joint_gain)
    turned_key = rotate(rotary_key.astype(jnp.float32), positions).astype(jnp.bfloat16)
    query_plain = jnp.dot(query_normed, query_weight, preferred_element_type=jnp.float32).astype(jnp.bfloat16)
    query_plain = query_plain.reshape(TOK_A, HEADS, NOPE)
    query_turned = jnp.dot(query_normed, query_rotary, preferred_element_type=jnp.float32)
    query_turned = rotate(query_turned.reshape(TOK_A, HEADS, ROPE), positions).astype(jnp.bfloat16)
    key_plain = jnp.dot(joint_normed, key_weight, preferred_element_type=jnp.float32).astype(jnp.bfloat16)
    key_plain = key_plain.reshape(TOK_A, HEADS, NOPE)
    values = jnp.dot(joint_normed, value_weight, preferred_element_type=jnp.float32).astype(jnp.bfloat16)
    values = values.reshape(TOK_A, HEADS, VDIM)
    score_scale = (NOPE + ROPE) ** (-0.5)

    def one_head(items_in):
        query_head, turned_head, key_head, value_head = items_in
        scores = jnp.dot(query_head, key_head.T, preferred_element_type=jnp.float32)
        scores = (scores + jnp.dot(turned_head, turned_key.T, preferred_element_type=jnp.float32)) * score_scale
        row_top = lax.optimization_barrier(jnp.max(scores, axis=-1, keepdims=True))
        expo = jnp.exp(scores - row_top)
        row_total = lax.optimization_barrier(jnp.sum(expo, axis=-1, keepdims=True))
        mixed_values = jnp.dot(expo.astype(jnp.bfloat16), value_head, preferred_element_type=jnp.float32)
        return (mixed_values / row_total).astype(jnp.bfloat16)
    per_head = lax.map(one_head, (query_plain.transpose(1, 0, 2), query_turned.transpose(1, 0, 2), key_plain.transpose(1, 0, 2), values.transpose(1, 0, 2)))
    attended = per_head.transpose(1, 0, 2).reshape(TOK_A, HEADS * VDIM)
    mixer_out = jnp.dot(attended, output_weight, preferred_element_type=jnp.float32).astype(jnp.bfloat16)
    expert_normed = norm_rows(expert_input, expert_gain)
    flat_routes = routes.reshape(-1).astype(jnp.int32)
    pair_count = TOK_B * TOPK
    owner_token = jnp.arange(pair_count, dtype=jnp.int32) // TOPK
    onehot = (flat_routes[:, None] == jnp.arange(EXPERTS, dtype=jnp.int32)[None, :]).astype(jnp.int32)
    rank_within = lax.optimization_barrier(jnp.sum((jnp.cumsum(onehot, axis=0) - onehot) * onehot, axis=1)).astype(jnp.int32)
    slot_width = N_EP * CAP
    slot_token = jnp.zeros((EXPERTS, slot_width), jnp.int32).at[flat_routes, rank_within].set(owner_token)
    block_width = FF // N_TP

    def one_expert(items_in):
        token_index, gate_matrix, up_matrix, down_matrix = items_in
        rows_in = expert_normed[token_index]
        gate_acts = jnp.dot(rows_in, gate_matrix, preferred_element_type=jnp.float32)
        up_acts = jnp.dot(rows_in, up_matrix, preferred_element_type=jnp.float32)
        hidden = (jax.nn.silu(gate_acts) * up_acts).astype(jnp.bfloat16)

        def add_block(running, block_index):
            start_at = (block_index * block_width).astype(jnp.int32)
            part_sum = jnp.dot(lax.dynamic_slice_in_dim(hidden, start_at, block_width, 1), lax.dynamic_slice_in_dim(down_matrix, start_at, block_width, 0), preferred_element_type=jnp.float32)
            part_sum = lax.optimization_barrier(part_sum.astype(jnp.bfloat16))
            return (running + part_sum.astype(jnp.float32), None)
        running, _ = lax.scan(add_block, jnp.zeros((slot_width, D), jnp.float32), jnp.arange(N_TP, dtype=jnp.int32))
        return running.astype(jnp.bfloat16)
    results = lax.map(one_expert, (slot_token, gate_weight, up_weight, down_weight))
    picked = results[flat_routes, rank_within].astype(jnp.float32).reshape(TOK_B, TOPK, D)
    expert_out = lax.optimization_barrier(jnp.sum(picked * route_weight[:, :, None], axis=1)).astype(jnp.bfloat16)
    return (mixer_out, expert_out)
```

```python
import functools

import jax
import jax.numpy as jnp
from jax import lax
from jax.experimental import pallas as pl
from jax.experimental.pallas import tpu as pltpu
from jax.sharding import PartitionSpec as P

NOPE = 64
VDIM = 64

NORM_EPSILON = 1e-06
ROTARY_BASE = 10000.0
F32 = jnp.float32
BF16 = jnp.bfloat16


def norm_rows(source, gain_vector):
    as_float = source.astype(F32)
    factor = lax.rsqrt(jnp.mean(as_float * as_float, axis=-1, keepdims=True) + NORM_EPSILON)
    return (as_float * factor * gain_vector).astype(BF16)


def rotation_tables(positions, width, copies):
    half_width = width // 2
    lane = jnp.arange(width * copies, dtype=jnp.int32) % width
    frequencies = ROTARY_BASE ** (-(lane % half_width).astype(F32) / half_width)
    angles = positions[:, None] * frequencies[None, :]
    sign = jnp.where(lane < half_width, -1.0, 1.0).astype(F32)
    return jnp.cos(angles), jnp.sin(angles) * sign[None, :]


def swap_matrix(width, copies):
    half_width = width // 2
    lane = jnp.arange(width * copies, dtype=jnp.int32)
    partner = (lane // width) * width + (lane % width + half_width) % width
    return (lane[:, None] == partner[None, :]).astype(BF16)


def attention_kernel(head_count, turn_width, scale, q_ref, qt_ref, kt_ref, tk_ref, v_ref, out_ref):
    turned_keys = tk_ref[...]
    pieces = []
    per_pair = 128 // VDIM
    for head in range(head_count):
        query = jnp.concatenate(
            [
                q_ref[:, head * NOPE : (head + 1) * NOPE],
                qt_ref[:, head * turn_width : (head + 1) * turn_width],
            ],
            axis=1,
        )
        keys = jnp.concatenate([kt_ref[head * NOPE : (head + 1) * NOPE, :], turned_keys], axis=0)
        scores = jnp.dot(query, keys, preferred_element_type=F32) * scale
        top = jnp.max(scores, axis=-1, keepdims=True)
        expo = jnp.exp(scores - top)
        total = jnp.sum(expo, axis=-1, keepdims=True)
        pair = head // per_pair
        mixed = jnp.dot(
            expo.astype(BF16), v_ref[:, pair * 128 : (pair + 1) * 128], preferred_element_type=F32
        )
        inner = head % per_pair
        mixed = mixed[:, inner * VDIM : (inner + 1) * VDIM]
        pieces.append((mixed / total).astype(BF16))
    out_ref[...] = jnp.concatenate(pieces, axis=1)


def attention(query_plain, query_turned, keys_t, turned_t, values, turn_width):
    rows, width = query_plain.shape
    tokens = values.shape[0]
    head_count = width // NOPE
    block = 128
    scale = (NOPE + turn_width) ** (-0.5)
    whole = lambda i: (0, 0)
    return pl.pallas_call(
        functools.partial(attention_kernel, head_count, turn_width, scale),
        grid=(rows // block,),
        in_specs=[
            pl.BlockSpec((block, width), lambda i: (i, 0)),
            pl.BlockSpec((block, query_turned.shape[1]), lambda i: (i, 0)),
            pl.BlockSpec(keys_t.shape, whole),
            pl.BlockSpec(turned_t.shape, whole),
            pl.BlockSpec(values.shape, whole),
        ],
        out_specs=pl.BlockSpec((block, head_count * VDIM), lambda i: (i, 0)),
        out_shape=jax.ShapeDtypeStruct((rows, head_count * VDIM), BF16),
        compiler_params=pltpu.CompilerParams(vmem_limit_bytes=40 * 1024 * 1024),
        cost_estimate=pl.CostEstimate(
            flops=40 * rows * tokens * head_count * (NOPE + turn_width),
            bytes_accessed=4 * tokens * width,
            transcendentals=rows * tokens * head_count,
        ),
        name="attention",
    )(query_plain, query_turned, keys_t, turned_t, values)


def half_of(source, parity, axis):
    half = source.shape[axis] // 2
    return lax.dynamic_slice_in_dim(source, parity * half, half, axis)


def swap_cores(source):
    size = lax.axis_size("tp")
    return lax.ppermute(source, "tp", [(i, i ^ 1) for i in range(size)])


def exchange(blocks, axis, stride, group):
    size = lax.axis_size(axis)
    me = (lax.axis_index(axis) // stride) % group
    own = lax.dynamic_index_in_dim(blocks, me, 0, keepdims=False)
    out = [own]
    for step in range(1, group):
        piece = lax.dynamic_index_in_dim(blocks, me ^ step, 0, keepdims=False)
        pairs = [(i, i ^ (step * stride)) for i in range(size)]
        out.append(lax.ppermute(piece, axis, pairs))
    return out


def gather(part, axis):
    size = lax.axis_size(axis)
    out = [part]
    for step in range(1, size):
        out.append(lax.ppermute(part, axis, [(i, i ^ step) for i in range(size)]))
    return out


def ordered(pieces, axis):
    me = lax.axis_index(axis)
    stacked = jnp.stack(pieces)
    return jnp.concatenate(
        [lax.dynamic_index_in_dim(stacked, me ^ i, 0, keepdims=False) for i in range(len(pieces))],
        axis=0,
    )


def sum_of(pieces):
    total = pieces[0].astype(F32)
    for piece in pieces[1:]:
        total = total + piece.astype(F32)
    return total.astype(BF16)


def latent_part(joint_latent, rotary_key, joint_gain, parity):
    row_count = joint_latent.shape[0]
    turn_width = rotary_key.shape[1]
    positions = (lax.axis_index("ep") * row_count + jnp.arange(row_count, dtype=jnp.int32)).astype(F32)
    normed = half_of(norm_rows(joint_latent, joint_gain), parity, 1)
    cosine, sine = rotation_tables(positions, turn_width, 1)
    swapped = jnp.dot(rotary_key, swap_matrix(turn_width, 1), preferred_element_type=F32)
    turned = (rotary_key.astype(F32) * cosine + swapped * sine).astype(BF16)
    return jnp.concatenate([normed, turned], axis=1)


def token_mixer(
    latent,
    query_latent,
    query_gain,
    query_weight,
    query_rotary,
    key_weight,
    value_weight,
    turn_width,
    parity,
):
    mine, other, turned = latent
    row_count = query_latent.shape[0]
    positions = (lax.axis_index("ep") * row_count + jnp.arange(row_count, dtype=jnp.int32)).astype(F32)
    head_count = key_weight.shape[1] // NOPE
    query_normed = norm_rows(query_latent, query_gain)
    query_plain = jnp.dot(query_normed, query_weight, preferred_element_type=F32).astype(BF16)
    cosine, sine = rotation_tables(positions, turn_width, head_count)
    rotary_swapped = jnp.dot(
        query_rotary, swap_matrix(turn_width, head_count), preferred_element_type=F32
    ).astype(BF16)
    query_turned = (
        jnp.dot(query_normed, query_rotary, preferred_element_type=F32) * cosine
        + jnp.dot(query_normed, rotary_swapped, preferred_element_type=F32) * sine
    ).astype(BF16)

    normed = jnp.where(
        parity == 0,
        jnp.concatenate([mine, other], axis=1),
        jnp.concatenate([other, mine], axis=1),
    )
    keys_t = jnp.einsum("td,df->ft", normed, key_weight, preferred_element_type=F32).astype(BF16)
    values = jnp.dot(normed, value_weight, preferred_element_type=F32).astype(BF16)
    return attention(query_plain, query_turned, keys_t, turned.T, values, turn_width)


def column_blocks(weight, parity, blocks):
    width = weight.shape[2] // blocks
    return jnp.concatenate(
        [
            lax.dynamic_slice_in_dim(weight, (2 * z + parity) * width, width, 2)
            for z in range(blocks // 2)
        ],
        axis=2,
    )


def local(
    query_latent,
    joint_latent,
    rotary_key,
    query_gain,
    joint_gain,
    query_weight,
    query_rotary,
    key_weight,
    value_weight,
    output_weight,
    expert_input,
    expert_gain,
    routes,
    route_weight,
    gate_weight,
    up_weight,
    down_weight,
):
    parity = lax.axis_index("tp") % 2
    tp_size = lax.axis_size("tp")
    row_count, feature_width = expert_input.shape
    group_count = lax.axis_size("ep")
    local_count = gate_weight.shape[0]
    expert_count = local_count * group_count
    capacity = 3 * row_count // (2 * group_count)
    half = feature_width // 2

    part = latent_part(joint_latent, rotary_key, joint_gain, parity)
    part, expert_rows = lax.optimization_barrier((part, expert_input))
    gathered = ordered(gather(part, "ep"), "ep")

    routes_t = routes.T
    names = jnp.arange(expert_count, dtype=jnp.int32)
    member = (routes_t[0][None, :] == names[:, None]) | (routes_t[1][None, :] == names[:, None])
    token = jnp.arange(row_count, dtype=jnp.int32)
    before = (token[:, None] < token[None, :]).astype(BF16)
    rank = jnp.dot(member.astype(BF16), before, preferred_element_type=F32).astype(jnp.int32)
    place = jnp.where(member, rank, -1)
    slots = jnp.arange(capacity, dtype=jnp.int32)
    chosen = (place[:, None, :] == slots[None, :, None]).astype(BF16)
    chosen = chosen.reshape(expert_count * capacity, row_count)
    rows_half = lax.optimization_barrier(half_of(norm_rows(expert_rows, expert_gain), parity, 1))
    outgoing = jnp.dot(chosen, rows_half, preferred_element_type=F32).astype(BF16)
    outgoing = outgoing.reshape(group_count, local_count, capacity, half)
    mine = jnp.stack(exchange(outgoing, "ep", 1, group_count))
    latent_half = gathered[:, : joint_latent.shape[1] // 2]
    attended = token_mixer(
        (latent_half, swap_cores(latent_half), gathered[:, joint_latent.shape[1] // 2 :]),
        query_latent,
        query_gain,
        query_weight,
        query_rotary,
        key_weight,
        value_weight,
        rotary_key.shape[1],
        parity,
    )
    mine, attended = lax.optimization_barrier((mine, attended))
    other = swap_cores(mine)
    partial = jnp.dot(attended, output_weight, preferred_element_type=F32).astype(BF16)
    partial = partial.reshape(tp_size // 2, 2, row_count // tp_size, feature_width)
    keep = lax.dynamic_index_in_dim(partial, parity, 1, keepdims=False)
    give = lax.dynamic_index_in_dim(partial, 1 - parity, 1, keepdims=False)
    paired = (keep.astype(F32) + swap_cores(give).astype(F32)).astype(BF16)
    mixer_out = sum_of(exchange(paired, "tp", 2, tp_size // 2))

    def project(weight):
        return jnp.einsum(
            "secd,edf->secf", mine, half_of(weight, parity, 1), preferred_element_type=F32
        ) + jnp.einsum(
            "secd,edf->secf", other, half_of(weight, 1 - parity, 1), preferred_element_type=F32
        )

    gate_acts = project(gate_weight)
    up_acts = project(up_weight)
    hidden = (jax.nn.silu(gate_acts) * up_acts).astype(BF16)

    def down(side):
        return jnp.einsum(
            "secf,efd->secd",
            hidden,
            column_blocks(down_weight, side, tp_size),
            preferred_element_type=F32,
        ).astype(BF16)

    theirs = swap_cores(down(1 - parity))
    summed = (down(parity).astype(F32) + theirs.astype(F32)).astype(BF16)
    back = [summed[0]]
    for step in range(1, group_count):
        back.append(lax.ppermute(summed[step], "ep", [(i, i ^ step) for i in range(group_count)]))
    back = [piece.reshape(local_count * capacity, half) for piece in back]
    returned = ordered(back, "ep")

    def picked(k):
        slot = jnp.sum(
            jnp.where(routes_t[k][None, :] == names[:, None], names[:, None] * capacity + rank, 0),
            axis=0,
        )
        every = jnp.arange(expert_count * capacity, dtype=jnp.int32)
        pick = (slot[:, None] == every[None, :]).astype(BF16)
        return jnp.dot(pick, returned, preferred_element_type=F32) * route_weight[:, k : k + 1]

    combined = (picked(0) + picked(1)).astype(BF16)
    combined = combined.reshape(row_count, tp_size // 2, half // (tp_size // 2)).transpose(1, 0, 2)
    expert_out = sum_of(exchange(combined, "tp", 2, tp_size // 2))
    return (mixer_out, expert_out)


def solution(mesh):
    return jax.shard_map(
        local,
        mesh=mesh,
        in_specs=(
            P("ep", None),
            P("ep", None),
            P("ep", None),
            P(),
            P(),
            P(None, "tp"),
            P(None, "tp"),
            P(None, "tp"),
            P(None, "tp"),
            P("tp", None),
            P("ep", None),
            P(),
            P("ep", None),
            P("ep", None),
            P("ep", None, "tp"),
            P("ep", None, "tp"),
            P("ep", "tp", None),
        ),
        out_specs=(P(("ep", "tp"), None), P("ep", "tp")),
        check_vma=False,
    )
```

```python
import functools
import math

import jax
import jax.numpy as jnp
import numpy as np
from jax import lax
from jax.experimental import pallas as pl
from jax.experimental.pallas import tpu as pltpu
from jax.sharding import PartitionSpec as P

NOPE = 64
VDIM = 64

NORM_EPSILON = 1e-06
ROTARY_BASE = 10000.0
F32 = jnp.float32
BF16 = jnp.bfloat16
MESH = pl.DeviceIdType.MESH
EARLY = 1


def xor(a, b, size):
    total, weight = 0, 1
    while weight < size:
        total = total + weight * ((a // weight + b // weight) % 2)
        weight *= 2
    return total


def dot(a, b):
    return jnp.dot(a, b, preferred_element_type=F32)


def dot_nt(a, b):
    return lax.dot_general(a, b, (((1,), (1,)), ((), ())), preferred_element_type=F32)


def iota(shape, axis):
    return lax.broadcasted_iota(jnp.int32, shape, axis)


def norm_factor(square_sum, width):
    return lax.rsqrt(square_sum * (1.0 / width) + NORM_EPSILON)


def kernel(
    dims,
    routes_ref,
    weights_ref,
    rotary_ref,
    freq_col_ref,
    freq_row_ref,
    query_gain_ref,
    joint_gain_ref,
    expert_gain_ref,
    query_latent_hbm,
    joint_hbm,
    query_weight_hbm,
    query_rotary_hbm,
    key_weight_hbm,
    value_weight_hbm,
    output_weight_hbm,
    expert_hbm,
    gate_hbm,
    up_hbm,
    down_hbm,
    mixer_ref,
    expert_out_ref,
    query_latent,
    joint,
    query_weight,
    query_rotary,
    key_weight,
    value_weight,
    output_weight,
    expert_in,
    gate,
    up,
    down,
    table,
    rows_half,
    outgoing,
    slots,
    pick,
    turned,
    queries,
    keys,
    values,
    attended,
    partial,
    mixer_pair,
    mixer_in,
    ours,
    theirs,
    arrived,
    returned,
    combined,
    combined_in,
    load_sem,
    joint_send,
    joint_recv,
    joint_core_send,
    joint_core_recv,
    turned_send,
    turned_recv,
    out_send,
    out_recv,
    core_send,
    core_recv,
    pair_send,
    pair_recv,
    mixer_send,
    mixer_recv,
    half_send,
    half_recv,
    back_send,
    back_recv,
    line_send,
    line_recv,
):
    n, m, rows, width, local_count, capacity, head_count, turn = dims
    nz = m // 2
    experts = n * local_count
    half = width // 2
    block_width = width // m
    row_block = rows // m
    hidden_width = gate.shape[2]
    latent_width = joint_hbm.shape[1]
    latent_half = latent_width // 2
    tokens = n * rows
    batch = local_count * capacity
    half_turn = turn // 2

    me = lax.axis_index("ep")
    t = lax.axis_index("tp")
    z = t // 2
    c = t % 2

    def at_ep(step):
        return (xor(me, step, n), t)

    def at_z(step):
        return (me, 2 * xor(z, step, nz) + c)

    partner = (me, 2 * z + 1 - c)

    def remote(src, dst, send, recv, where):
        return pltpu.make_async_remote_copy(
            src_ref=src, dst_ref=dst, send_sem=send, recv_sem=recv, device_id=where, device_id_type=MESH
        )

    loads = [
        pltpu.make_async_copy(src, dst, load_sem.at[i])
        for i, (src, dst) in enumerate(
            [
                (expert_hbm, expert_in),
                (joint_hbm.at[:, pl.ds(0, latent_half)], joint.at[0, 0]),
                (joint_hbm.at[:, pl.ds(latent_half, latent_half)], joint.at[1, 0]),
                (query_latent_hbm, query_latent),
                (query_weight_hbm, query_weight),
                (query_rotary_hbm, query_rotary),
                (key_weight_hbm, key_weight),
                (value_weight_hbm, value_weight),
                (output_weight_hbm, output_weight),
                (gate_hbm, gate),
                (up_hbm, up),
                (down_hbm, down),
            ]
        )
    ]
    for load in loads:
        load.start()

    barrier = pltpu.get_barrier_semaphore()
    peers = [at_ep(step) for step in range(1, n)] + [at_z(step) for step in range(1, nz)] + [partner]
    for peer in peers:
        pl.semaphore_signal(barrier, inc=1, device_id=peer, device_id_type=MESH)
    pl.semaphore_wait(barrier, len(peers))

    joint_half = joint_hbm.at[:, pl.ds(pl.multiple_of(c * latent_half, latent_half), latent_half)]
    joint_copies = [
        remote(joint_half, joint.at[c, step], joint_send.at[step], joint_recv.at[step], at_ep(step))
        for step in range(1, n)
    ]
    for copy in joint_copies:
        copy.start()

    position = (me * rows + iota((half_turn, rows), 1)).astype(F32)
    angle = position * freq_col_ref[...]
    cosine, sine = jnp.cos(angle), jnp.sin(angle)
    first = rotary_ref[0:half_turn, :].astype(F32)
    second = rotary_ref[half_turn:turn, :].astype(F32)
    turned[0] = jnp.concatenate(
        [first * cosine - second * sine, second * cosine + first * sine], axis=0
    ).astype(BF16)

    names = iota((experts, rows), 0)
    first_member = routes_ref[0:1, :] == names
    second_member = routes_ref[1:2, :] == names
    member = first_member | second_member
    before = (iota((rows, rows), 0) < iota((rows, rows), 1)).astype(BF16)
    rank = dot(member.astype(BF16), before)
    place = jnp.where(member, rank, -4096.0)
    share = jnp.where(first_member, weights_ref[0:1, :], 0.0) + jnp.where(
        second_member, weights_ref[1:2, :], 0.0
    )
    table[...] = jnp.zeros_like(table)
    for group in range(n):
        span = slice(group * local_count, (group + 1) * local_count)
        table[group, 0:local_count, :] = place[span, :]
        table[group, local_count : 2 * local_count, :] = share[span, :]

    turned_copies = [
        remote(turned.at[0], turned.at[step], turned_send.at[step], turned_recv.at[step], at_ep(step))
        for step in range(1, n)
    ]
    for copy in turned_copies:
        copy.start()

    loads[0].wait()
    piece = 128 if rows % 128 == 0 else rows
    own_columns = pl.ds(pl.multiple_of(c * half, half), half)

    @pl.loop(0, rows // piece)
    def _(i):
        span = pl.ds(pl.multiple_of(i * piece, piece), piece)
        whole = expert_in[span, :].astype(F32)
        factor = norm_factor(jnp.sum(whole * whole, axis=-1, keepdims=True), width)
        part = expert_in[span, own_columns].astype(F32)
        rows_half[span, :] = (part * factor * expert_gain_ref[:, own_columns]).astype(BF16)

    def chosen(step, expert):
        group = xor(me, step, n)
        spots = table[group, expert : expert + 1, :]
        hit = iota((capacity, rows), 0).astype(F32) == spots
        return dot(hit.astype(BF16), rows_half[...]).astype(BF16)

    out_copies = []
    for step in range(1, n):
        for expert in range(local_count):
            outgoing[step - 1, expert] = chosen(step, expert)
        copy = remote(
            outgoing.at[step - 1],
            slots.at[c, :, pl.ds(step * capacity, capacity), :],
            out_send.at[step],
            out_recv.at[step],
            at_ep(step),
        )
        copy.start()
        out_copies.append(copy)
    for expert in range(local_count):
        slots[c, expert, 0:capacity, :] = chosen(0, expert)

    def core_copy(step):
        where = (c, slice(None), pl.ds(step * capacity, capacity), slice(None))
        return remote(slots.at[where], slots.at[where], core_send.at[step], core_recv.at[step], partner)

    core_copies = [core_copy(step) for step in range(n)]
    core_copies[0].start()

    same = (iota((rows, rows), 0) == iota((rows, rows), 1)).astype(BF16)

    @pl.loop(0, n)
    def _(step):
        group = xor(me, step, n)
        upright = dot_nt(same, table[group].astype(BF16))
        lane = iota((rows, batch), 1).astype(F32)
        total = jnp.zeros((rows, batch), F32)
        for expert in range(local_count):
            spot = upright[:, expert : expert + 1] + float(expert * capacity)
            gain = upright[:, local_count + expert : local_count + expert + 1]
            total = total + jnp.where(lane == spot, gain, 0.0)
        pick[step] = total.astype(BF16)

    for i in (3, 4, 5):
        loads[i].wait()
    turn_width = head_count * turn
    lane = iota((turn_width, turn_width), 0)
    other = iota((turn_width, turn_width), 1)
    other = (other // turn) * turn + (other % turn + half_turn) % turn
    swapped = dot(query_rotary[...], (lane == other).astype(BF16)).astype(BF16)
    query_width = query_latent.shape[1]

    @pl.loop(0, rows // piece)
    def _(i):
        span = pl.ds(pl.multiple_of(i * piece, piece), piece)
        source = query_latent[span, :].astype(F32)
        factor = norm_factor(jnp.sum(source * source, axis=-1, keepdims=True), query_width)
        normed = (source * factor * query_gain_ref[...]).astype(BF16)
        plain = dot(normed, query_weight[...]).astype(BF16)
        at = (me * rows + i * piece + iota((piece, turn_width), 0)).astype(F32) * freq_row_ref[...]
        sign = jnp.where(iota((piece, turn_width), 1) % turn < half_turn, -1.0, 1.0)
        spun = dot(normed, query_rotary[...]) * jnp.cos(at) + dot(normed, swapped) * (jnp.sin(at) * sign)
        spun = spun.astype(BF16)
        for head in range(head_count):
            queries[head, span, :] = jnp.concatenate(
                [plain[:, head * NOPE : (head + 1) * NOPE], spun[:, head * turn : (head + 1) * turn]],
                axis=1,
            )

    def joint_core(step):
        here = joint.at[c, step]
        return remote(here, here, joint_core_send.at[step], joint_core_recv.at[step], partner)

    joint_cores = [joint_core(step) for step in range(1, n)]
    for i in (1, 2, 6, 7):
        loads[i].wait()
    key_turned = jnp.transpose(key_weight[...].astype(F32)).astype(BF16)

    def keys_of(step):
        left = joint[0, step].astype(F32)
        right = joint[1, step].astype(F32)
        square = jnp.sum(left * left, axis=-1, keepdims=True) + jnp.sum(right * right, axis=-1, keepdims=True)
        factor = norm_factor(square, latent_width)
        left = (left * factor * joint_gain_ref[:, 0:latent_half]).astype(BF16)
        right = (right * factor * joint_gain_ref[:, latent_half:latent_width]).astype(BF16)
        normed = jnp.concatenate([left, right], axis=1)
        upright = dot_nt(key_turned, normed).astype(BF16)
        columns = slice(step * rows, (step + 1) * rows)
        for head in range(head_count):
            keys[head, 0:NOPE, columns] = upright[head * NOPE : (head + 1) * NOPE, :]
            keys[head, NOPE : NOPE + turn, columns] = turned[step]
        values[columns, :] = dot(normed, value_weight[...]).astype(BF16)

    keys_of(0)
    for step in range(1, n):
        joint_copies[step - 1].wait_recv()
        joint_cores[step - 1].start()
    for step in range(1, n):
        turned_copies[step - 1].wait_recv()
        joint_cores[step - 1].wait_recv()
        keys_of(step)

    scale = (NOPE + turn) ** (-0.5) * math.log2(math.e)
    query_block = max(32, min(rows, 128 * 2048 // tokens))
    per_pair = 128 // VDIM

    @pl.loop(0, rows // query_block)
    def _(i):
        span = pl.ds(pl.multiple_of(i * query_block, query_block), query_block)
        pieces = []
        for head in range(head_count):
            scores = dot(queries[head, span, :], keys[head])
            top = jnp.max(scores, axis=-1, keepdims=True)
            expo = jnp.exp2((scores - top) * scale)
            total = jnp.sum(expo, axis=-1, keepdims=True)
            pair = head // per_pair
            mixed = dot(expo.astype(BF16), values[:, pair * 128 : (pair + 1) * 128])
            inner = head % per_pair
            pieces.append((mixed[:, inner * VDIM : (inner + 1) * VDIM] / total).astype(BF16))
        attended[span, :] = jnp.concatenate(pieces, axis=1)

    loads[8].wait()
    chunk = 512

    @pl.loop(0, width // chunk)
    def _(i):
        columns = pl.ds(pl.multiple_of(i * chunk, chunk), chunk)
        product = dot(attended[...], output_weight[:, columns]).astype(BF16)
        partial[:, :, columns] = product.reshape(m, row_block, chunk)

    pair_copies = [
        remote(partial.at[2 * i + 1 - c], mixer_pair.at[i], pair_send.at[i], pair_recv.at[i], partner)
        for i in range(nz)
    ]
    for copy in pair_copies:
        copy.start()

    for step in range(1, n - 1):
        out_copies[step - 1].wait_recv()
        core_copies[step].start()

    for i in range(nz):
        pair_copies[i].wait_recv()
        both = partial[2 * i + c].astype(F32) + mixer_pair[i].astype(F32)
        mixer_pair[i] = both.astype(BF16)
    mixer_copies = [
        remote(
            mixer_pair.at[xor(z, step, nz)],
            mixer_in.at[step],
            mixer_send.at[step],
            mixer_recv.at[step],
            at_z(step),
        )
        for step in range(1, nz)
    ]
    for copy in mixer_copies[::-1]:
        copy.start()

    for i in (9, 10, 11):
        loads[i].wait()

    def experts_on(low, high):
        count = (high - low) * capacity
        span = slice(low * capacity, high * capacity)

        @pl.loop(0, local_count)
        def _(expert):
            left = slots[0, expert, span, :]
            right = slots[1, expert, span, :]
            gate_acts = dot(left, gate[expert, 0:half, :]) + dot(right, gate[expert, half:width, :])
            up_acts = dot(left, up[expert, 0:half, :]) + dot(right, up[expert, half:width, :])
            hidden = (gate_acts / (1.0 + jnp.exp(-gate_acts)) * up_acts).astype(BF16)
            for turn_index in range(nz):
                block = xor(z, nz - 1 - turn_index, nz)
                mine = pl.ds(pl.multiple_of((2 * block + c) * block_width, block_width), block_width)
                yours = pl.ds(pl.multiple_of((2 * block + 1 - c) * block_width, block_width), block_width)
                theirs[turn_index, expert, span, :] = dot(hidden, down[expert, :, yours]).astype(BF16)
                ours[turn_index, expert, span, :] = dot(hidden, down[expert, :, mine]).astype(BF16)

    def half_copy(stage, turn_index, low, high):
        where = (turn_index, slice(None), pl.ds(low * capacity, (high - low) * capacity), slice(None))
        return remote(
            theirs.at[where],
            arrived.at[where],
            half_send.at[stage, turn_index],
            half_recv.at[stage, turn_index],
            partner,
        )

    def add_halves(turn_index, low, high):
        for expert in range(local_count):
            span = slice(low * capacity, high * capacity)
            both = ours[turn_index, expert, span, :].astype(F32) + arrived[turn_index, expert, span, :].astype(F32)
            ours[turn_index, expert, span, :] = both.astype(BF16)

    def back_copy(turn_index, step):
        return remote(
            ours.at[turn_index, :, pl.ds(step * capacity, capacity), :],
            returned.at[turn_index, step],
            back_send.at[turn_index, step],
            back_recv.at[turn_index, step],
            at_ep(step),
        )

    back_copies = [[back_copy(q, step) for step in range(1, n)] for q in range(nz)]

    core_copies[0].wait_recv()
    for step in range(1, n - 1):
        core_copies[step].wait_recv()
    experts_on(0, n - 1)
    first_halves = [half_copy(0, q, 0, n - 1) for q in range(nz)]
    for copy in first_halves:
        copy.start()
    out_copies[n - 2].wait_recv()
    core_copies[n - 1].start()
    for q in range(nz):
        first_halves[q].wait_recv()
        add_halves(q, 0, n - 1)
        if q < EARLY:
            for step in range(1, n - 1):
                back_copies[q][step - 1].start()
    core_copies[n - 1].wait_recv()
    experts_on(n - 1, n)
    last_halves = [half_copy(1, q, n - 1, n) for q in range(nz)]
    for copy in last_halves:
        copy.start()
    for q in range(nz):
        last_halves[q].wait_recv()
        add_halves(q, n - 1, n)
        for step in range(1, n):
            if step == n - 1 or q >= EARLY:
                back_copies[q][step - 1].start()

    total = mixer_pair[z].astype(F32)
    for step in range(1, nz):
        mixer_copies[step - 1].wait_recv()
        total = total + mixer_in[step].astype(F32)
    mixer_ref[...] = total.astype(BF16)

    line_copies = []
    last = None
    for q in range(nz):
        own = ours[q, :, 0:capacity, :].reshape(batch, block_width)
        last = dot(pick[0], own)
        for step in range(1, n):
            back_copies[q][step - 1].wait_recv()
            last = last + dot(pick[step], returned[q, step].reshape(batch, block_width))
        if q < nz - 1:
            combined[q] = last.astype(BF16)
            step = nz - 1 - q
            copy = remote(combined.at[q], combined_in.at[step], line_send.at[step], line_recv.at[step], at_z(step))
            copy.start()
            line_copies.append(copy)
    for step in range(nz - 1, 0, -1):
        line_copies[nz - 1 - step].wait_recv()
        last = last + combined_in[step].astype(F32)
    expert_out_ref[...] = last.astype(BF16)

    sent = joint_copies + turned_copies + out_copies + core_copies + joint_cores + pair_copies
    sent = sent + mixer_copies + first_halves + last_halves + line_copies
    for copies in back_copies:
        sent = sent + copies
    for copy in sent:
        copy.wait_send()


def local(
    query_latent,
    joint_latent,
    rotary_key,
    query_gain,
    joint_gain,
    query_weight,
    query_rotary,
    key_weight,
    value_weight,
    output_weight,
    expert_input,
    expert_gain,
    routes,
    route_weight,
    gate_weight,
    up_weight,
    down_weight,
):
    n = lax.axis_size("ep")
    m = lax.axis_size("tp")
    nz = m // 2
    rows, width = expert_input.shape
    local_count = gate_weight.shape[0]
    capacity = 3 * rows // (2 * n)
    turn = rotary_key.shape[1]
    half_turn = turn // 2
    head_count = key_weight.shape[1] // NOPE
    latent_half = joint_latent.shape[1] // 2
    tokens = n * rows
    batch = local_count * capacity
    block_width = width // m
    row_block = rows // m
    half = width // 2
    dims = (n, m, rows, width, local_count, capacity, head_count, turn)

    powers = (ROTARY_BASE ** (-np.arange(half_turn) / half_turn)).astype(np.float32)
    freq_col = jnp.asarray(powers[:, None])
    freq_row = jnp.asarray(np.tile(powers, 2 * head_count)[None, :])

    small = [
        routes.T,
        route_weight.T,
        rotary_key.T,
        freq_col,
        freq_row,
        query_gain[None, :],
        joint_gain[None, :],
        expert_gain[None, :],
    ]
    large = [
        query_latent,
        joint_latent,
        query_weight,
        query_rotary,
        key_weight,
        value_weight,
        output_weight,
        expert_input,
        gate_weight,
        up_weight,
        down_weight,
    ]

    def like(source):
        return pltpu.VMEM(source.shape, source.dtype)

    def buffer(*shape):
        return pltpu.VMEM(shape, BF16)

    dma = pltpu.SemaphoreType.DMA
    scratch = [
        like(query_latent),
        buffer(2, n, rows, latent_half),
        like(query_weight),
        like(query_rotary),
        like(key_weight),
        like(value_weight),
        like(output_weight),
        like(expert_input),
        like(gate_weight),
        like(up_weight),
        like(down_weight),
        pltpu.VMEM((n, 8, rows), F32),
        buffer(rows, half),
        buffer(n - 1, local_count, capacity, half),
        buffer(2, local_count, n * capacity, half),
        buffer(n, rows, batch),
        buffer(n, turn, rows),
        buffer(head_count, rows, NOPE + turn),
        buffer(head_count, NOPE + turn, tokens),
        buffer(tokens, head_count * VDIM),
        buffer(rows, head_count * VDIM),
        buffer(m, row_block, width),
        buffer(nz, row_block, width),
        buffer(nz, row_block, width),
        buffer(nz, local_count, n * capacity, block_width),
        buffer(nz, local_count, n * capacity, block_width),
        buffer(nz, local_count, n * capacity, block_width),
        buffer(nz, n, local_count, capacity, block_width),
        buffer(nz - 1, rows, block_width),
        buffer(nz, rows, block_width),
        dma((12,)),
    ]
    for shape in ((n,), (n,), (n,), (n,), (n,), (nz,), (nz,), (2, nz), (nz, n), (nz,)):
        scratch += [dma(shape), dma(shape)]

    vmem = pl.BlockSpec(memory_space=pltpu.VMEM)
    anywhere = pl.BlockSpec(memory_space=pl.ANY)
    return pl.pallas_call(
        functools.partial(kernel, dims),
        in_specs=[vmem] * len(small) + [anywhere] * len(large),
        out_specs=(vmem, vmem),
        out_shape=(
            jax.ShapeDtypeStruct((row_block, width), BF16),
            jax.ShapeDtypeStruct((rows, block_width), BF16),
        ),
        scratch_shapes=scratch,
        compiler_params=pltpu.CompilerParams(
            collective_id=0, has_side_effects=True, vmem_limit_bytes=67043328
        ),
        name="whole",
    )(*small, *large)


def solution(mesh):
    return jax.shard_map(
        local,
        mesh=mesh,
        in_specs=(
            P("ep", None),
            P("ep", None),
            P("ep", None),
            P(),
            P(),
            P(None, "tp"),
            P(None, "tp"),
            P(None, "tp"),
            P(None, "tp"),
            P("tp", None),
            P("ep", None),
            P(),
            P("ep", None),
            P("ep", None),
            P("ep", None, "tp"),
            P("ep", None, "tp"),
            P("ep", "tp", None),
        ),
        out_specs=(P(("ep", "tp"), None), P("ep", "tp")),
        check_vma=False,
    )
```

```python
import functools
import math

import jax
import jax.numpy as jnp
import numpy as np
from jax import lax
from jax.experimental import pallas as pl
from jax.experimental.pallas import tpu as pltpu
from jax.sharding import PartitionSpec as P

NOPE = 64
VDIM = 64

NORM_EPSILON = 1e-06
ROTARY_BASE = 10000.0
F32 = jnp.float32
BF16 = jnp.bfloat16
MESH = pl.DeviceIdType.MESH
EARLY = 1
AHEAD = 2
SHARED_EIGHTHS = 2


def xor(a, b, size):
    total, weight = 0, 1
    while weight < size:
        total = total + weight * ((a // weight + b // weight) % 2)
        weight *= 2
    return total


def low_bit(value):
    return value & -value


def line_order(size):
    return list(range(size - 1, -1, -1))


def line_sources(x, size):
    limit = low_bit(x) if x else size
    return [x ^ (1 << i) for i in range(size.bit_length()) if (1 << i) < limit]


def dot(a, b):
    return jnp.dot(a, b, preferred_element_type=F32)


def dot_nt(a, b):
    return lax.dot_general(a, b, (((1,), (1,)), ((), ())), preferred_element_type=F32)


def iota(shape, axis):
    return lax.broadcasted_iota(jnp.int32, shape, axis)


def norm_factor(square_sum, width):
    return lax.rsqrt(square_sum * (1.0 / width) + NORM_EPSILON)


def kernel(
    dims,
    routes_ref,
    weights_ref,
    rotary_ref,
    freq_col_ref,
    freq_row_ref,
    query_gain_ref,
    joint_gain_ref,
    expert_gain_ref,
    query_latent_hbm,
    joint_hbm,
    query_weight_hbm,
    query_rotary_hbm,
    key_weight_hbm,
    value_weight_hbm,
    output_weight_hbm,
    expert_hbm,
    gate_hbm,
    up_hbm,
    down_hbm,
    mixer_ref,
    expert_out_ref,
    query_latent,
    joint,
    query_weight,
    query_rotary,
    key_weight,
    value_weight,
    output_weight,
    expert_in,
    gate,
    up,
    down,
    table,
    rows_half,
    outgoing,
    outgoing_both,
    slots,
    pick,
    turned,
    queries,
    keys,
    values,
    attended,
    partial,
    mixer_pair,
    mixer_in,
    ours,
    theirs,
    arrived,
    returned,
    combined,
    combined_in,
    load_sem,
    joint_send,
    joint_recv,
    joint_line_send,
    joint_line_recv,
    joint_core_send,
    joint_core_recv,
    turned_send,
    turned_recv,
    out_send,
    out_recv,
    both_send,
    both_recv,
    share_send,
    share_recv,
    core_send,
    core_recv,
    pair_send,
    pair_recv,
    mixer_send,
    mixer_recv,
    half_send,
    half_recv,
    back_send,
    back_recv,
    line_send,
    line_recv,
):
    n, m, rows, width, local_count, capacity, head_count, turn = dims
    nz = m // 2
    experts = n * local_count
    half = width // 2
    block_width = width // m
    row_block = rows // m
    hidden_width = gate.shape[2]
    latent_width = joint_hbm.shape[1]
    latent_half = latent_width // 2
    tokens = n * rows
    batch = local_count * capacity
    half_turn = turn // 2

    me = lax.axis_index("ep")
    t = lax.axis_index("tp")
    z = t // 2
    c = t % 2
    parity = z % 2
    order = line_order(nz)

    def at_ep(step):
        return (xor(me, step, n), t)

    def at_z(step):
        return (me, 2 * xor(z, step, nz) + c)

    partner = (me, 2 * z + 1 - c)

    def remote(src, dst, send, recv, where):
        return pltpu.make_async_remote_copy(
            src_ref=src, dst_ref=dst, send_sem=send, recv_sem=recv, device_id=where, device_id_type=MESH
        )

    loads = [
        pltpu.make_async_copy(src, dst, load_sem.at[i])
        for i, (src, dst) in enumerate(
            [
                (expert_hbm, expert_in),
                (joint_hbm.at[:, pl.ds(0, latent_half)], joint.at[0, 0]),
                (joint_hbm.at[:, pl.ds(latent_half, latent_half)], joint.at[1, 0]),
                (query_latent_hbm, query_latent),
                (query_weight_hbm, query_weight),
                (query_rotary_hbm, query_rotary),
                (key_weight_hbm, key_weight),
                (value_weight_hbm, value_weight),
                (output_weight_hbm, output_weight),
                (gate_hbm, gate),
                (up_hbm, up),
                (down_hbm, down),
            ]
        )
    ]
    for load in loads:
        load.start()

    barrier = pltpu.get_barrier_semaphore()
    peers = [at_ep(step) for step in range(1, n)] + [at_z(step) for step in range(1, nz)] + [partner]
    for peer in peers:
        pl.semaphore_signal(barrier, inc=1, device_id=peer, device_id_type=MESH)
    pl.semaphore_wait(barrier, len(peers))

    quarter = latent_half // 2
    lanes_mine = pl.ds(pl.multiple_of(parity * quarter, quarter), quarter)
    lanes_other = pl.ds(pl.multiple_of((1 - parity) * quarter, quarter), quarter)
    first_lane = c * latent_half + parity * quarter
    joint_part = joint_hbm.at[:, pl.ds(pl.multiple_of(first_lane, quarter), quarter)]

    joint_copies = [
        remote(
            joint_part,
            joint.at[c, step, :, lanes_mine],
            joint_send.at[step],
            joint_recv.at[step],
            at_ep(step),
        )
        for step in range(1, n)
    ]

    def joint_line(step):
        here = joint.at[c, step, :, lanes_mine]
        return remote(here, here, joint_line_send.at[step], joint_line_recv.at[step], at_z(1))

    def joint_core(kind, step):
        here = joint.at[c, step, :, lanes_other if kind else lanes_mine]
        return remote(here, here, joint_core_send.at[kind, step], joint_core_recv.at[kind, step], partner)

    joint_lines = [joint_line(step) for step in range(1, n)]
    joint_cores = [[joint_core(kind, step) for step in range(1, n)] for kind in range(2)]
    for copy in joint_copies[:-1]:
        copy.start()

    def pass_joint(step):
        joint_copies[step - 1].wait_recv()
        joint_lines[step - 1].start()
        joint_cores[0][step - 1].start()

    def pass_joint_line(step):
        joint_lines[step - 1].wait_recv()
        joint_cores[1][step - 1].start()

    position = (me * rows + iota((half_turn, rows), 1)).astype(F32)
    angle = position * freq_col_ref[...]
    cosine, sine = jnp.cos(angle), jnp.sin(angle)
    first = rotary_ref[0:half_turn, :].astype(F32)
    second = rotary_ref[half_turn:turn, :].astype(F32)
    turned[0] = jnp.concatenate(
        [first * cosine - second * sine, second * cosine + first * sine], axis=0
    ).astype(BF16)

    names = iota((experts, rows), 0)
    first_member = routes_ref[0:1, :] == names
    second_member = routes_ref[1:2, :] == names
    member = first_member | second_member
    before = (iota((rows, rows), 0) < iota((rows, rows), 1)).astype(BF16)
    rank = dot(member.astype(BF16), before)
    place = jnp.where(member, rank, -4096.0)
    share = jnp.where(first_member, weights_ref[0:1, :], 0.0) + jnp.where(
        second_member, weights_ref[1:2, :], 0.0
    )
    table[...] = jnp.zeros_like(table)
    for group in range(n):
        span = slice(group * local_count, (group + 1) * local_count)
        table[group, 0:local_count, :] = place[span, :]
        table[group, local_count : 2 * local_count, :] = share[span, :]

    turned_copies = [
        remote(turned.at[0], turned.at[step], turned_send.at[step], turned_recv.at[step], at_ep(step))
        for step in range(1, n)
    ]
    for copy in turned_copies:
        copy.start()

    loads[0].wait()
    piece = 128 if rows % 128 == 0 else rows
    own_columns = pl.ds(pl.multiple_of(c * half, half), half)

    @pl.loop(0, rows // piece)
    def _(i):
        span = pl.ds(pl.multiple_of(i * piece, piece), piece)
        whole = expert_in[span, :].astype(F32)
        factor = norm_factor(jnp.sum(whole * whole, axis=-1, keepdims=True), width)
        part = expert_in[span, own_columns].astype(F32)
        rows_half[span, :] = (part * factor * expert_gain_ref[:, own_columns]).astype(BF16)

    joint_copies[-1].start()

    shared = half * SHARED_EIGHTHS // 8
    share_mine = pl.ds(pl.multiple_of(parity * shared, shared), shared)
    share_other = pl.ds(pl.multiple_of((1 - parity) * shared, shared), shared)
    both_lanes = pl.ds(2 * shared, half - 2 * shared)

    def chosen(step, expert, columns):
        group = xor(me, step, n)
        spots = table[group, expert : expert + 1, :]
        hit = iota((capacity, rows), 0).astype(F32) == spots
        return dot(hit.astype(BF16), rows_half[:, columns]).astype(BF16)

    def slots_at(step, lanes):
        return slots.at[c, :, pl.ds(step * capacity, capacity), lanes]

    out_copies = []
    for step in range(1, n):
        for expert in range(local_count):
            outgoing[step - 1, expert] = chosen(step, expert, share_mine)
        copy = remote(
            outgoing.at[step - 1],
            slots_at(step, share_mine),
            out_send.at[step],
            out_recv.at[step],
            at_ep(step),
        )
        out_copies.append(copy)
    both_copies = []
    for step in range(1, n):
        for expert in range(local_count):
            outgoing_both[step - 1, expert] = chosen(step, expert, both_lanes)
        copy = remote(
            outgoing_both.at[step - 1],
            slots_at(step, both_lanes),
            both_send.at[step],
            both_recv.at[step],
            at_ep(step),
        )
        both_copies.append(copy)

    def share_copy(step):
        here = slots_at(step, share_mine)
        return remote(here, here, share_send.at[step], share_recv.at[step], at_z(1))

    def core_copy(kind, step):
        here = slots_at(step, (share_mine, share_other, both_lanes)[kind])
        return remote(here, here, core_send.at[kind, step], core_recv.at[kind, step], partner)

    share_copies = [share_copy(step) for step in range(1, n)]
    core_copies = [[core_copy(kind, step) for step in range(n)] for kind in range(3)]

    def pass_out(step):
        out_copies[step - 1].wait_recv()
        share_copies[step - 1].start()
        core_copies[0][step].start()

    def pass_share(step):
        share_copies[step - 1].wait_recv()
        core_copies[1][step].start()

    def pass_both(step):
        both_copies[step - 1].wait_recv()
        core_copies[2][step].start()

    def wait_core(step):
        for kind in range(3):
            core_copies[kind][step].wait_recv()

    for expert in range(local_count):
        slots[c, expert, 0:capacity, :] = chosen(0, expert, slice(None))
    for kind in range(3):
        core_copies[kind][0].start()
    for step in range(1, n - 1):
        pass_joint(step)
    for copy in out_copies[:-1]:
        copy.start()
    for copy in both_copies[:-1]:
        copy.start()

    for i in (3, 4, 5):
        loads[i].wait()
    turn_width = head_count * turn
    lane = iota((turn_width, turn_width), 0)
    other = iota((turn_width, turn_width), 1)
    other = (other // turn) * turn + (other % turn + half_turn) % turn
    swapped = dot(query_rotary[...], (lane == other).astype(BF16)).astype(BF16)
    query_width = query_latent.shape[1]

    @pl.loop(0, rows // piece)
    def _(i):
        span = pl.ds(pl.multiple_of(i * piece, piece), piece)
        source = query_latent[span, :].astype(F32)
        factor = norm_factor(jnp.sum(source * source, axis=-1, keepdims=True), query_width)
        normed = (source * factor * query_gain_ref[...]).astype(BF16)
        plain = dot(normed, query_weight[...]).astype(BF16)
        at = (me * rows + i * piece + iota((piece, turn_width), 0)).astype(F32) * freq_row_ref[...]
        sign = jnp.where(iota((piece, turn_width), 1) % turn < half_turn, -1.0, 1.0)
        spun = dot(normed, query_rotary[...]) * jnp.cos(at) + dot(normed, swapped) * (jnp.sin(at) * sign)
        spun = spun.astype(BF16)
        for head in range(head_count):
            queries[head, span, :] = jnp.concatenate(
                [plain[:, head * NOPE : (head + 1) * NOPE], spun[:, head * turn : (head + 1) * turn]],
                axis=1,
            )

    for i in (9, 10, 11):
        loads[i].wait()

    def experts_on(low, high, first, last):
        count = (high - low) * capacity
        span = slice(low * capacity, high * capacity)

        @pl.loop(first, last)
        def _(expert):
            left = slots[0, expert, span, :]
            right = slots[1, expert, span, :]
            gate_acts = dot(left, gate[expert, 0:half, :]) + dot(right, gate[expert, half:width, :])
            up_acts = dot(left, up[expert, 0:half, :]) + dot(right, up[expert, half:width, :])
            hidden = (gate_acts / (1.0 + jnp.exp(-gate_acts)) * up_acts).astype(BF16)
            for turn_index in range(nz):
                block = xor(z, order[turn_index], nz)
                mine = pl.ds(pl.multiple_of((2 * block + c) * block_width, block_width), block_width)
                yours = pl.ds(pl.multiple_of((2 * block + 1 - c) * block_width, block_width), block_width)
                theirs[turn_index, expert, span, :] = dot(hidden, down[expert, :, yours]).astype(BF16)
                ours[turn_index, expert, span, :] = dot(hidden, down[expert, :, mine]).astype(BF16)

    stages = [(0, 1), (1, n - 1), (n - 1, n)]

    def half_copy(stage, expert):
        low, high = stages[stage]
        where = (slice(None), expert, pl.ds(low * capacity, (high - low) * capacity), slice(None))
        return remote(
            theirs.at[where],
            arrived.at[where],
            half_send.at[stage, expert],
            half_recv.at[stage, expert],
            partner,
        )

    half_copies = [[half_copy(stage, expert) for expert in range(local_count)] for stage in range(3)]

    def add_halves(turn_index, low, high):
        for expert in range(local_count):
            span = slice(low * capacity, high * capacity)
            both = ours[turn_index, expert, span, :].astype(F32) + arrived[turn_index, expert, span, :].astype(F32)
            ours[turn_index, expert, span, :] = both.astype(BF16)

    def back_copy(turn_index, step):
        return remote(
            ours.at[turn_index, :, pl.ds(step * capacity, capacity), :],
            returned.at[turn_index, step],
            back_send.at[turn_index, step],
            back_recv.at[turn_index, step],
            at_ep(step),
        )

    back_copies = [[back_copy(q, step) for step in range(1, n)] for q in range(nz)]

    pass_joint(n - 1)
    out_copies[-1].start()
    wait_core(0)
    experts_on(0, 1, 0, local_count)
    for expert in range(local_count):
        half_copies[0][expert].start()

    for i in (1, 2, 6, 7):
        loads[i].wait()
    key_turned = jnp.transpose(key_weight[...].astype(F32)).astype(BF16)

    def keys_of(step):
        left = joint[0, step].astype(F32)
        right = joint[1, step].astype(F32)
        square = jnp.sum(left * left, axis=-1, keepdims=True) + jnp.sum(right * right, axis=-1, keepdims=True)
        factor = norm_factor(square, latent_width)
        left = (left * factor * joint_gain_ref[:, 0:latent_half]).astype(BF16)
        right = (right * factor * joint_gain_ref[:, latent_half:latent_width]).astype(BF16)
        normed = jnp.concatenate([left, right], axis=1)
        upright = dot_nt(key_turned, normed).astype(BF16)
        columns = slice(step * rows, (step + 1) * rows)
        for head in range(head_count):
            keys[head, 0:NOPE, columns] = upright[head * NOPE : (head + 1) * NOPE, :]
            keys[head, NOPE : NOPE + turn, columns] = turned[step]
        values[columns, :] = dot(normed, value_weight[...]).astype(BF16)

    both_copies[-1].start()
    keys_of(0)
    for step in range(1, n - 1):
        pass_joint_line(step)
    for step in range(1, n - 1):
        pass_out(step)
    pass_joint_line(n - 1)
    for step in range(1, n):
        turned_copies[step - 1].wait_recv()
        joint_cores[0][step - 1].wait_recv()
        joint_cores[1][step - 1].wait_recv()
        keys_of(step)

    scale = (NOPE + turn) ** (-0.5) * math.log2(math.e)
    line_rows = 2 * row_block
    query_block = max(32, min(line_rows, 128 * 2048 // tokens))
    per_pair = 128 // VDIM

    def attend(first, i):
        span = pl.ds(pl.multiple_of(first + i * query_block, query_block), query_block)
        pieces = []
        for head in range(head_count):
            scores = dot(queries[head, span, :], keys[head])
            top = jnp.max(scores, axis=-1, keepdims=True)
            expo = jnp.exp2((scores - top) * scale)
            total = jnp.sum(expo, axis=-1, keepdims=True)
            pair = head // per_pair
            mixed = dot(expo.astype(BF16), values[:, pair * 128 : (pair + 1) * 128])
            inner = head % per_pair
            pieces.append((mixed[:, inner * VDIM : (inner + 1) * VDIM] / total).astype(BF16))
        attended[span, :] = jnp.concatenate(pieces, axis=1)

    chunk = 512

    def attend_line(x):
        first = xor(z, x, nz) * line_rows
        pl.loop(0, line_rows // query_block)(functools.partial(attend, first))

    def project_line(x):
        block = xor(z, x, nz)
        span = pl.ds(pl.multiple_of(block * line_rows, line_rows), line_rows)

        @pl.loop(0, width // chunk)
        def _(i):
            columns = pl.ds(pl.multiple_of(i * chunk, chunk), chunk)
            product = dot(attended[span, :], output_weight[:, columns]).astype(BF16)
            partial[pl.ds(2 * block, 2), :, columns] = product.reshape(2, row_block, chunk)

    def pair_copy(x):
        block = xor(z, x, nz)
        return remote(
            partial.at[2 * block + 1 - c], mixer_pair.at[block], pair_send.at[x], pair_recv.at[x], partner
        )

    pair_copies = [pair_copy(x) for x in range(nz)]

    def pair_sum(x):
        block = xor(z, x, nz)
        pair_copies[x].wait_recv()
        both = partial[2 * block + c].astype(F32) + mixer_pair[block].astype(F32)
        mixer_pair[block] = both.astype(BF16)

    for x in order[:-1]:
        attend_line(x)
    loads[8].wait()
    for x in order[:-1]:
        project_line(x)
        pair_copies[x].start()

    for step in range(1, n - 1):
        pass_both(step)
    for step in range(1, n - 1):
        pass_share(step)
    pass_out(n - 1)

    def mixer_copy(x):
        block = mixer_pair.at[xor(z, x, nz)]
        return remote(block, mixer_in.at[x], mixer_send.at[x], mixer_recv.at[x], at_z(low_bit(x)))

    mixer_copies = {x: mixer_copy(x) for x in order[:-1]}

    def mixer_sum(x):
        block = xor(z, x, nz)
        total = mixer_pair[block].astype(F32)
        for source in line_sources(x, nz):
            mixer_copies[source].wait_recv()
            total = total + mixer_in[source].astype(F32)
        return total

    def mixer_first():
        for x in order[:-1]:
            pair_sum(x)
            if low_bit(x) == 1:
                mixer_copies[x].start()

    def mixer_next(bit):
        for x in order[:-1]:
            if low_bit(x) == bit:
                mixer_pair[xor(z, x, nz)] = mixer_sum(x).astype(BF16)
                mixer_copies[x].start()


    mixer_first()
    for step in range(1, n - 1):
        wait_core(step)
    for expert in range(local_count):
        experts_on(1, n - 1, expert, expert + 1)
        half_copies[1][expert].start()
        if expert == 0:
            pass_both(n - 1)
            pass_share(n - 1)
    wait_core(n - 1)
    for expert in range(local_count):
        experts_on(n - 1, n, expert, expert + 1)
        half_copies[2][expert].start()
        if expert == 0:
            for stage in range(2):
                for copy in half_copies[stage]:
                    copy.wait_recv()
            for q in range(EARLY):
                add_halves(q, 0, n - 1)
                for step in range(1, n - 1):
                    back_copies[q][step - 1].start()
    for q in range(EARLY, nz):
        add_halves(q, 0, n - 1)
    for copy in half_copies[2]:
        copy.wait_recv()
    def send_back(q):
        for step in range(1, n):
            if step == n - 1 or q >= EARLY:
                back_copies[q][step - 1].start()

    for q in range(nz):
        add_halves(q, n - 1, n)
        if q < AHEAD:
            send_back(q)

    same = (iota((rows, rows), 0) == iota((rows, rows), 1)).astype(BF16)

    @pl.loop(0, n)
    def _(step):
        group = xor(me, step, n)
        upright = dot_nt(same, table[group].astype(BF16))
        lane = iota((rows, batch), 1).astype(F32)
        total = jnp.zeros((rows, batch), F32)
        for expert in range(local_count):
            spot = upright[:, expert : expert + 1] + float(expert * capacity)
            gain = upright[:, local_count + expert : local_count + expert + 1]
            total = total + jnp.where(lane == spot, gain, 0.0)
        pick[step] = total.astype(BF16)


    attend_line(0)
    project_line(0)
    pair_copies[0].start()

    bit = 2
    while bit < nz:
        mixer_next(bit)
        bit *= 2

    def line_copy(q):
        x = order[q]
        return remote(combined.at[q], combined_in.at[x], line_send.at[x], line_recv.at[x], at_z(low_bit(x)))

    line_copies = {order[q]: line_copy(q) for q in range(nz - 1)}
    for q in range(nz):
        x = order[q]
        own = ours[q, :, 0:capacity, :].reshape(batch, block_width)
        total = dot(pick[0], own)
        for step in range(1, n):
            back_copies[q][step - 1].wait_recv()
            total = total + dot(pick[step], returned[q, step].reshape(batch, block_width))
        if x == 0:
            pair_sum(0)
            mixer_ref[...] = mixer_sum(0).astype(BF16)
        for source in line_sources(x, nz):
            line_copies[source].wait_recv()
            total = total + combined_in[source].astype(F32)
        if x:
            combined[q] = total.astype(BF16)
            line_copies[x].start()
            if q + AHEAD < nz:
                send_back(q + AHEAD)
        else:
            expert_out_ref[...] = total.astype(BF16)

    sent = joint_copies + joint_lines + joint_cores[0] + joint_cores[1] + turned_copies
    sent = sent + out_copies + both_copies + share_copies + pair_copies
    for copies in core_copies + back_copies + half_copies:
        sent = sent + copies
    sent = sent + [mixer_copies[x] for x in order[:-1]] + [line_copies[x] for x in order[:-1]]
    for copy in sent:
        copy.wait_send()


def local(
    query_latent,
    joint_latent,
    rotary_key,
    query_gain,
    joint_gain,
    query_weight,
    query_rotary,
    key_weight,
    value_weight,
    output_weight,
    expert_input,
    expert_gain,
    routes,
    route_weight,
    gate_weight,
    up_weight,
    down_weight,
):
    n = lax.axis_size("ep")
    m = lax.axis_size("tp")
    nz = m // 2
    rows, width = expert_input.shape
    local_count = gate_weight.shape[0]
    capacity = 3 * rows // (2 * n)
    turn = rotary_key.shape[1]
    half_turn = turn // 2
    head_count = key_weight.shape[1] // NOPE
    latent_half = joint_latent.shape[1] // 2
    tokens = n * rows
    batch = local_count * capacity
    block_width = width // m
    row_block = rows // m
    half = width // 2
    dims = (n, m, rows, width, local_count, capacity, head_count, turn)

    powers = (ROTARY_BASE ** (-np.arange(half_turn) / half_turn)).astype(np.float32)
    freq_col = jnp.asarray(powers[:, None])
    freq_row = jnp.asarray(np.tile(powers, 2 * head_count)[None, :])

    small = [
        routes.T,
        route_weight.T,
        rotary_key.T,
        freq_col,
        freq_row,
        query_gain[None, :],
        joint_gain[None, :],
        expert_gain[None, :],
    ]
    large = [
        query_latent,
        joint_latent,
        query_weight,
        query_rotary,
        key_weight,
        value_weight,
        output_weight,
        expert_input,
        gate_weight,
        up_weight,
        down_weight,
    ]

    def like(source):
        return pltpu.VMEM(source.shape, source.dtype)

    def buffer(*shape):
        return pltpu.VMEM(shape, BF16)

    dma = pltpu.SemaphoreType.DMA
    scratch = [
        like(query_latent),
        buffer(2, n, rows, latent_half),
        like(query_weight),
        like(query_rotary),
        like(key_weight),
        like(value_weight),
        like(output_weight),
        like(expert_input),
        like(gate_weight),
        like(up_weight),
        like(down_weight),
        pltpu.VMEM((n, 8, rows), F32),
        buffer(rows, half),
        buffer(n - 1, local_count, capacity, half * SHARED_EIGHTHS // 8),
        buffer(n - 1, local_count, capacity, half - 2 * (half * SHARED_EIGHTHS // 8)),
        buffer(2, local_count, n * capacity, half),
        buffer(n, rows, batch),
        buffer(n, turn, rows),
        buffer(head_count, rows, NOPE + turn),
        buffer(head_count, NOPE + turn, tokens),
        buffer(tokens, head_count * VDIM),
        buffer(rows, head_count * VDIM),
        buffer(m, row_block, width),
        buffer(nz, row_block, width),
        buffer(nz, row_block, width),
        buffer(nz, local_count, n * capacity, block_width),
        buffer(nz, local_count, n * capacity, block_width),
        buffer(nz, local_count, n * capacity, block_width),
        buffer(nz, n, local_count, capacity, block_width),
        buffer(nz - 1, rows, block_width),
        buffer(nz, rows, block_width),
        dma((12,)),
    ]
    line = [(n,), (n,), (2, n), (n,), (n,), (n,), (n,), (3, n), (nz,), (nz,), (3, local_count), (nz, n), (nz,)]
    for shape in line:
        scratch += [dma(shape), dma(shape)]

    vmem = pl.BlockSpec(memory_space=pltpu.VMEM)
    anywhere = pl.BlockSpec(memory_space=pl.ANY)
    return pl.pallas_call(
        functools.partial(kernel, dims),
        in_specs=[vmem] * len(small) + [anywhere] * len(large),
        out_specs=(vmem, vmem),
        out_shape=(
            jax.ShapeDtypeStruct((row_block, width), BF16),
            jax.ShapeDtypeStruct((rows, block_width), BF16),
        ),
        scratch_shapes=scratch,
        compiler_params=pltpu.CompilerParams(
            collective_id=0, has_side_effects=True, vmem_limit_bytes=67043328
        ),
        name="whole",
    )(*small, *large)


def solution(mesh):
    return jax.shard_map(
        local,
        mesh=mesh,
        in_specs=(
            P("ep", None),
            P("ep", None),
            P("ep", None),
            P(),
            P(),
            P(None, "tp"),
            P(None, "tp"),
            P(None, "tp"),
            P(None, "tp"),
            P("tp", None),
            P("ep", None),
            P(),
            P("ep", None),
            P("ep", None),
            P("ep", None, "tp"),
            P("ep", None, "tp"),
            P("ep", "tp", None),
        ),
        out_specs=(P(("ep", "tp"), None), P("ep", "tp")),
        check_vma=False,
    )
```

```python
import functools
import math

import jax
import jax.numpy as jnp
import numpy as np
from jax import lax
from jax.experimental import pallas as pl
from jax.experimental.pallas import tpu as pltpu
from jax.sharding import PartitionSpec as P

NOPE = 64
VDIM = 64

NORM_EPSILON = 1e-06
ROTARY_BASE = 10000.0
F32 = jnp.float32
BF16 = jnp.bfloat16
MESH = pl.DeviceIdType.MESH
EARLY = 1
AHEAD = 2
SHARED_EIGHTHS = 2


def xor(a, b, size):
    total, weight = 0, 1
    while weight < size:
        total = total + weight * ((a // weight + b // weight) % 2)
        weight *= 2
    return total


def low_bit(value):
    return value & -value


def line_order(size):
    return list(range(size - 1, -1, -1))


def line_sources(x, size):
    limit = low_bit(x) if x else size
    return [x ^ (1 << i) for i in range(size.bit_length()) if (1 << i) < limit]


def dot(a, b):
    return jnp.dot(a, b, preferred_element_type=F32)


def dot_nt(a, b):
    return lax.dot_general(a, b, (((1,), (1,)), ((), ())), preferred_element_type=F32)


def iota(shape, axis):
    return lax.broadcasted_iota(jnp.int32, shape, axis)


def norm_factor(square_sum, width):
    return lax.rsqrt(square_sum * (1.0 / width) + NORM_EPSILON)


def kernel(
    dims,
    routes_ref,
    weights_ref,
    rotary_ref,
    freq_col_ref,
    freq_row_ref,
    query_gain_ref,
    joint_gain_ref,
    expert_gain_ref,
    query_latent_hbm,
    joint_hbm,
    query_weight_hbm,
    query_rotary_hbm,
    key_weight_hbm,
    value_weight_hbm,
    output_weight_hbm,
    expert_hbm,
    gate_hbm,
    up_hbm,
    down_hbm,
    mixer_ref,
    expert_out_ref,
    query_latent,
    joint,
    query_weight,
    query_rotary,
    key_weight,
    value_weight,
    output_weight,
    expert_in,
    gate,
    up,
    down,
    table,
    rows_half,
    outgoing,
    outgoing_both,
    slots,
    pick,
    turned,
    queries,
    keys,
    values,
    attended,
    partial,
    mixer_pair,
    mixer_in,
    ours,
    theirs,
    arrived,
    returned,
    combined,
    combined_in,
    load_sem,
    joint_send,
    joint_recv,
    joint_line_send,
    joint_line_recv,
    joint_core_send,
    joint_core_recv,
    turned_send,
    turned_recv,
    out_send,
    out_recv,
    both_send,
    both_recv,
    share_send,
    share_recv,
    core_send,
    core_recv,
    pair_send,
    pair_recv,
    mixer_send,
    mixer_recv,
    half_send,
    half_recv,
    back_send,
    back_recv,
    line_send,
    line_recv,
):
    n, m, rows, width, local_count, capacity, head_count, turn = dims
    nz = m // 2
    experts = n * local_count
    half = width // 2
    block_width = width // m
    row_block = rows // m
    hidden_width = gate.shape[2]
    latent_width = joint_hbm.shape[1]
    latent_half = latent_width // 2
    tokens = n * rows
    batch = local_count * capacity
    half_turn = turn // 2

    me = lax.axis_index("ep")
    t = lax.axis_index("tp")
    z = t // 2
    c = t % 2
    parity = z % 2
    order = line_order(nz)

    def at_ep(step):
        return (xor(me, step, n), t)

    def at_z(step):
        return (me, 2 * xor(z, step, nz) + c)

    partner = (me, 2 * z + 1 - c)

    def remote(src, dst, send, recv, where):
        return pltpu.make_async_remote_copy(
            src_ref=src, dst_ref=dst, send_sem=send, recv_sem=recv, device_id=where, device_id_type=MESH
        )

    loads = [
        pltpu.make_async_copy(src, dst, load_sem.at[i])
        for i, (src, dst) in enumerate(
            [
                (expert_hbm, expert_in),
                (joint_hbm.at[:, pl.ds(0, latent_half)], joint.at[0, 0]),
                (joint_hbm.at[:, pl.ds(latent_half, latent_half)], joint.at[1, 0]),
                (query_latent_hbm, query_latent),
                (query_weight_hbm, query_weight),
                (query_rotary_hbm, query_rotary),
                (key_weight_hbm, key_weight),
                (value_weight_hbm, value_weight),
                (output_weight_hbm, output_weight),
                (gate_hbm, gate),
                (up_hbm, up),
                (down_hbm, down),
            ]
        )
    ]
    for load in loads:
        load.start()

    barrier = pltpu.get_barrier_semaphore()
    peers = [at_ep(step) for step in range(1, n)] + [at_z(step) for step in range(1, nz)] + [partner]
    for peer in peers:
        pl.semaphore_signal(barrier, inc=1, device_id=peer, device_id_type=MESH)
    pl.semaphore_wait(barrier, len(peers))

    quarter = latent_half // 2
    lanes_mine = pl.ds(pl.multiple_of(parity * quarter, quarter), quarter)
    lanes_other = pl.ds(pl.multiple_of((1 - parity) * quarter, quarter), quarter)
    first_lane = c * latent_half + parity * quarter
    joint_part = joint_hbm.at[:, pl.ds(pl.multiple_of(first_lane, quarter), quarter)]

    joint_copies = [
        remote(
            joint_part,
            joint.at[c, step, :, lanes_mine],
            joint_send.at[step],
            joint_recv.at[step],
            at_ep(step),
        )
        for step in range(1, n)
    ]

    def joint_line(step):
        here = joint.at[c, step, :, lanes_mine]
        return remote(here, here, joint_line_send.at[step], joint_line_recv.at[step], at_z(1))

    def joint_core(kind, step):
        here = joint.at[c, step, :, lanes_other if kind else lanes_mine]
        return remote(here, here, joint_core_send.at[kind, step], joint_core_recv.at[kind, step], partner)

    joint_lines = [joint_line(step) for step in range(1, n)]
    joint_cores = [[joint_core(kind, step) for step in range(1, n)] for kind in range(2)]
    for copy in joint_copies[:-1]:
        copy.start()

    def pass_joint(step):
        joint_copies[step - 1].wait_recv()
        joint_lines[step - 1].start()
        joint_cores[0][step - 1].start()

    def pass_joint_line(step):
        joint_lines[step - 1].wait_recv()
        joint_cores[1][step - 1].start()

    position = (me * rows + iota((half_turn, rows), 1)).astype(F32)
    angle = position * freq_col_ref[...]
    cosine, sine = jnp.cos(angle), jnp.sin(angle)
    first = rotary_ref[0:half_turn, :].astype(F32)
    second = rotary_ref[half_turn:turn, :].astype(F32)
    turned[0] = jnp.concatenate(
        [first * cosine - second * sine, second * cosine + first * sine], axis=0
    ).astype(BF16)

    names = iota((experts, rows), 0)
    first_member = routes_ref[0:1, :] == names
    second_member = routes_ref[1:2, :] == names
    member = first_member | second_member
    before = (iota((rows, rows), 0) < iota((rows, rows), 1)).astype(BF16)
    rank = dot(member.astype(BF16), before)
    place = jnp.where(member, rank, -4096.0)
    share = jnp.where(first_member, weights_ref[0:1, :], 0.0) + jnp.where(
        second_member, weights_ref[1:2, :], 0.0
    )
    table[...] = jnp.zeros_like(table)
    for group in range(n):
        span = slice(group * local_count, (group + 1) * local_count)
        table[group, 0:local_count, :] = place[span, :]
        table[group, local_count : 2 * local_count, :] = share[span, :]

    turned_copies = [
        remote(turned.at[0], turned.at[step], turned_send.at[step], turned_recv.at[step], at_ep(step))
        for step in range(1, n)
    ]
    for copy in turned_copies:
        copy.start()

    loads[0].wait()
    piece = 128 if rows % 128 == 0 else rows
    own_columns = pl.ds(pl.multiple_of(c * half, half), half)

    @pl.loop(0, rows // piece)
    def _(i):
        span = pl.ds(pl.multiple_of(i * piece, piece), piece)
        whole = expert_in[span, :].astype(F32)
        factor = norm_factor(jnp.sum(whole * whole, axis=-1, keepdims=True), width)
        part = expert_in[span, own_columns].astype(F32)
        rows_half[span, :] = (part * factor * expert_gain_ref[:, own_columns]).astype(BF16)

    joint_copies[-1].start()

    shared = half * SHARED_EIGHTHS // 8
    share_mine = pl.ds(pl.multiple_of(parity * shared, shared), shared)
    share_other = pl.ds(pl.multiple_of((1 - parity) * shared, shared), shared)
    both_lanes = pl.ds(2 * shared, half - 2 * shared)

    def chosen(step, expert, columns):
        group = xor(me, step, n)
        spots = table[group, expert : expert + 1, :]
        hit = iota((capacity, rows), 0).astype(F32) == spots
        return dot(hit.astype(BF16), rows_half[:, columns]).astype(BF16)

    def slots_at(step, lanes):
        return slots.at[c, :, pl.ds(step * capacity, capacity), lanes]

    out_copies = []
    for step in range(1, n):
        for expert in range(local_count):
            outgoing[step - 1, expert] = chosen(step, expert, share_mine)
        copy = remote(
            outgoing.at[step - 1],
            slots_at(step, share_mine),
            out_send.at[step],
            out_recv.at[step],
            at_ep(step),
        )
        out_copies.append(copy)
    both_copies = []
    for step in range(1, n):
        for expert in range(local_count):
            outgoing_both[step - 1, expert] = chosen(step, expert, both_lanes)
        copy = remote(
            outgoing_both.at[step - 1],
            slots_at(step, both_lanes),
            both_send.at[step],
            both_recv.at[step],
            at_ep(step),
        )
        both_copies.append(copy)

    def share_copy(step):
        here = slots_at(step, share_mine)
        return remote(here, here, share_send.at[step], share_recv.at[step], at_z(1))

    def core_copy(kind, step):
        here = slots_at(step, (share_mine, share_other, both_lanes)[kind])
        return remote(here, here, core_send.at[kind, step], core_recv.at[kind, step], partner)

    share_copies = [share_copy(step) for step in range(1, n)]
    core_copies = [[core_copy(kind, step) for step in range(n)] for kind in range(3)]

    def pass_out(step):
        out_copies[step - 1].wait_recv()
        share_copies[step - 1].start()
        core_copies[0][step].start()

    def pass_share(step):
        share_copies[step - 1].wait_recv()
        core_copies[1][step].start()

    def pass_both(step):
        both_copies[step - 1].wait_recv()
        core_copies[2][step].start()

    def wait_core(step):
        for kind in range(3):
            core_copies[kind][step].wait_recv()

    for expert in range(local_count):
        slots[c, expert, 0:capacity, :] = chosen(0, expert, slice(None))
    for kind in range(3):
        core_copies[kind][0].start()
    for step in range(1, n - 1):
        pass_joint(step)
    for copy in out_copies[:-1]:
        copy.start()
    for copy in both_copies[:-1]:
        copy.start()

    for i in (3, 4, 5):
        loads[i].wait()
    turn_width = head_count * turn
    lane = iota((turn_width, turn_width), 0)
    other = iota((turn_width, turn_width), 1)
    other = (other // turn) * turn + (other % turn + half_turn) % turn
    swapped = dot(query_rotary[...], (lane == other).astype(BF16)).astype(BF16)
    query_width = query_latent.shape[1]

    @pl.loop(0, rows // piece)
    def _(i):
        span = pl.ds(pl.multiple_of(i * piece, piece), piece)
        source = query_latent[span, :].astype(F32)
        factor = norm_factor(jnp.sum(source * source, axis=-1, keepdims=True), query_width)
        normed = (source * factor * query_gain_ref[...]).astype(BF16)
        plain = dot(normed, query_weight[...]).astype(BF16)
        at = (me * rows + i * piece + iota((piece, turn_width), 0)).astype(F32) * freq_row_ref[...]
        sign = jnp.where(iota((piece, turn_width), 1) % turn < half_turn, -1.0, 1.0)
        spun = dot(normed, query_rotary[...]) * jnp.cos(at) + dot(normed, swapped) * (jnp.sin(at) * sign)
        spun = spun.astype(BF16)
        for head in range(head_count):
            queries[head, span, :] = jnp.concatenate(
                [plain[:, head * NOPE : (head + 1) * NOPE], spun[:, head * turn : (head + 1) * turn]],
                axis=1,
            )

    for i in (9, 10, 11):
        loads[i].wait()

    def experts_on(low, high, first, last):
        count = (high - low) * capacity
        span = slice(low * capacity, high * capacity)

        @pl.loop(first, last)
        def _(expert):
            left = slots[0, expert, span, :]
            right = slots[1, expert, span, :]
            gate_acts = dot(left, gate[expert, 0:half, :]) + dot(right, gate[expert, half:width, :])
            up_acts = dot(left, up[expert, 0:half, :]) + dot(right, up[expert, half:width, :])
            hidden = (gate_acts / (1.0 + jnp.exp(-gate_acts)) * up_acts).astype(BF16)
            for turn_index in range(nz):
                block = xor(z, order[turn_index], nz)
                mine = pl.ds(pl.multiple_of((2 * block + c) * block_width, block_width), block_width)
                yours = pl.ds(pl.multiple_of((2 * block + 1 - c) * block_width, block_width), block_width)
                theirs[turn_index, expert, span, :] = dot(hidden, down[expert, :, yours]).astype(BF16)
                ours[turn_index, expert, span, :] = dot(hidden, down[expert, :, mine]).astype(BF16)

    stages = [(0, 1), (1, n - 1), (n - 1, n)]

    def half_copy(stage, expert):
        low, high = stages[stage]
        where = (slice(None), expert, pl.ds(low * capacity, (high - low) * capacity), slice(None))
        return remote(
            theirs.at[where],
            arrived.at[where],
            half_send.at[stage, expert],
            half_recv.at[stage, expert],
            partner,
        )

    half_copies = [[half_copy(stage, expert) for expert in range(local_count)] for stage in range(3)]

    def add_halves(turn_index, low, high):
        for expert in range(local_count):
            span = slice(low * capacity, high * capacity)
            both = ours[turn_index, expert, span, :].astype(F32) + arrived[turn_index, expert, span, :].astype(F32)
            ours[turn_index, expert, span, :] = both.astype(BF16)

    def back_copy(turn_index, step):
        return remote(
            ours.at[turn_index, :, pl.ds(step * capacity, capacity), :],
            returned.at[turn_index, step],
            back_send.at[turn_index, step],
            back_recv.at[turn_index, step],
            at_ep(step),
        )

    back_copies = [[back_copy(q, step) for step in range(1, n)] for q in range(nz)]

    pass_joint(n - 1)
    out_copies[-1].start()
    wait_core(0)
    experts_on(0, 1, 0, local_count)
    for expert in range(local_count):
        half_copies[0][expert].start()

    for i in (1, 2, 6, 7):
        loads[i].wait()
    key_turned = jnp.transpose(key_weight[...].astype(F32)).astype(BF16)

    def keys_of(step):
        left = joint[0, step].astype(F32)
        right = joint[1, step].astype(F32)
        square = jnp.sum(left * left, axis=-1, keepdims=True) + jnp.sum(right * right, axis=-1, keepdims=True)
        factor = norm_factor(square, latent_width)
        left = (left * factor * joint_gain_ref[:, 0:latent_half]).astype(BF16)
        right = (right * factor * joint_gain_ref[:, latent_half:latent_width]).astype(BF16)
        normed = jnp.concatenate([left, right], axis=1)
        upright = dot_nt(key_turned, normed).astype(BF16)
        columns = slice(step * rows, (step + 1) * rows)
        for head in range(head_count):
            keys[head, 0:NOPE, columns] = upright[head * NOPE : (head + 1) * NOPE, :]
            keys[head, NOPE : NOPE + turn, columns] = turned[step]
        values[columns, :] = dot(normed, value_weight[...]).astype(BF16)

    both_copies[-1].start()
    keys_of(0)
    for step in range(1, n - 1):
        pass_joint_line(step)
    for step in range(1, n - 1):
        pass_out(step)
    pass_joint_line(n - 1)
    for step in range(1, n):
        turned_copies[step - 1].wait_recv()
        joint_cores[0][step - 1].wait_recv()
        joint_cores[1][step - 1].wait_recv()
        keys_of(step)

    scale = (NOPE + turn) ** (-0.5) * math.log2(math.e)
    line_rows = 2 * row_block
    query_block = max(32, min(line_rows, 128 * 2048 // tokens))
    per_pair = 128 // VDIM

    def attend(first, i):
        span = pl.ds(pl.multiple_of(first + i * query_block, query_block), query_block)
        pieces = []
        for head in range(head_count):
            scores = dot(queries[head, span, :], keys[head])
            top = jnp.max(scores, axis=-1, keepdims=True)
            expo = jnp.exp2((scores - top) * scale)
            total = jnp.sum(expo, axis=-1, keepdims=True)
            pair = head // per_pair
            mixed = dot(expo.astype(BF16), values[:, pair * 128 : (pair + 1) * 128])
            inner = head % per_pair
            pieces.append((mixed[:, inner * VDIM : (inner + 1) * VDIM] / total).astype(BF16))
        attended[span, :] = jnp.concatenate(pieces, axis=1)

    chunk = 512

    def attend_line(x):
        first = xor(z, x, nz) * line_rows
        pl.loop(0, line_rows // query_block)(functools.partial(attend, first))

    def project_line(x):
        block = xor(z, x, nz)
        span = pl.ds(pl.multiple_of(block * line_rows, line_rows), line_rows)

        @pl.loop(0, width // chunk)
        def _(i):
            columns = pl.ds(pl.multiple_of(i * chunk, chunk), chunk)
            product = dot(attended[span, :], output_weight[:, columns]).astype(BF16)
            partial[pl.ds(2 * block, 2), :, columns] = product.reshape(2, row_block, chunk)

    def pair_copy(x):
        block = xor(z, x, nz)
        return remote(
            partial.at[2 * block + 1 - c], mixer_pair.at[block], pair_send.at[x], pair_recv.at[x], partner
        )

    pair_copies = [pair_copy(x) for x in range(nz)]

    def pair_sum(x):
        block = xor(z, x, nz)
        pair_copies[x].wait_recv()
        both = partial[2 * block + c].astype(F32) + mixer_pair[block].astype(F32)
        mixer_pair[block] = both.astype(BF16)

    for i, x in enumerate(order[:-1]):
        attend_line(x)
        if i == nz // 2 - 1:
            pass_out(n - 1)
    for step in range(1, n - 1):
        pass_both(step)
    loads[8].wait()
    for x in order[:-1]:
        project_line(x)
        pair_copies[x].start()

    for step in range(1, n - 1):
        pass_share(step)

    def mixer_copy(x):
        block = mixer_pair.at[xor(z, x, nz)]
        return remote(block, mixer_in.at[x], mixer_send.at[x], mixer_recv.at[x], at_z(low_bit(x)))

    mixer_copies = {x: mixer_copy(x) for x in order[:-1]}

    def mixer_sum(x):
        block = xor(z, x, nz)
        total = mixer_pair[block].astype(F32)
        for source in line_sources(x, nz):
            mixer_copies[source].wait_recv()
            total = total + mixer_in[source].astype(F32)
        return total

    def mixer_first():
        for x in order[:-1]:
            pair_sum(x)
            if low_bit(x) == 1:
                mixer_copies[x].start()

    def mixer_next(bit):
        for x in order[:-1]:
            if low_bit(x) == bit:
                mixer_pair[xor(z, x, nz)] = mixer_sum(x).astype(BF16)
                mixer_copies[x].start()


    mixer_first()
    for step in range(1, n - 1):
        wait_core(step)
    for expert in range(local_count):
        experts_on(1, n - 1, expert, expert + 1)
        half_copies[1][expert].start()
        if expert == 0:
            pass_both(n - 1)
            pass_share(n - 1)
    wait_core(n - 1)
    for expert in range(local_count):
        experts_on(n - 1, n, expert, expert + 1)
        half_copies[2][expert].start()
        if expert == 0:
            for stage in range(2):
                for copy in half_copies[stage]:
                    copy.wait_recv()
            for q in range(EARLY):
                add_halves(q, 0, n - 1)
                for step in range(1, n - 1):
                    back_copies[q][step - 1].start()
    for q in range(EARLY, nz):
        add_halves(q, 0, n - 1)
    for copy in half_copies[2]:
        copy.wait_recv()
    def send_back(q):
        for step in range(1, n):
            if step == n - 1 or q >= EARLY:
                back_copies[q][step - 1].start()

    for q in range(nz):
        add_halves(q, n - 1, n)
        if q < AHEAD:
            send_back(q)

    same = (iota((rows, rows), 0) == iota((rows, rows), 1)).astype(BF16)

    @pl.loop(0, n)
    def _(step):
        group = xor(me, step, n)
        upright = dot_nt(same, table[group].astype(BF16))
        lane = iota((rows, batch), 1).astype(F32)
        total = jnp.zeros((rows, batch), F32)
        for expert in range(local_count):
            spot = upright[:, expert : expert + 1] + float(expert * capacity)
            gain = upright[:, local_count + expert : local_count + expert + 1]
            total = total + jnp.where(lane == spot, gain, 0.0)
        pick[step] = total.astype(BF16)


    attend_line(0)
    project_line(0)
    pair_copies[0].start()

    bit = 2
    while bit < nz:
        mixer_next(bit)
        bit *= 2

    def line_copy(q):
        x = order[q]
        return remote(combined.at[q], combined_in.at[x], line_send.at[x], line_recv.at[x], at_z(low_bit(x)))

    line_copies = {order[q]: line_copy(q) for q in range(nz - 1)}
    for q in range(nz):
        x = order[q]
        own = ours[q, :, 0:capacity, :].reshape(batch, block_width)
        total = dot(pick[0], own)
        for step in range(1, n):
            back_copies[q][step - 1].wait_recv()
            total = total + dot(pick[step], returned[q, step].reshape(batch, block_width))
        if x == 0:
            pair_sum(0)
            mixer_ref[...] = mixer_sum(0).astype(BF16)
        for source in line_sources(x, nz):
            line_copies[source].wait_recv()
            total = total + combined_in[source].astype(F32)
        if x:
            combined[q] = total.astype(BF16)
            line_copies[x].start()
            if q + AHEAD < nz:
                send_back(q + AHEAD)
        else:
            expert_out_ref[...] = total.astype(BF16)

    sent = joint_copies + joint_lines + joint_cores[0] + joint_cores[1] + turned_copies
    sent = sent + out_copies + both_copies + share_copies + pair_copies
    for copies in core_copies + back_copies + half_copies:
        sent = sent + copies
    sent = sent + [mixer_copies[x] for x in order[:-1]] + [line_copies[x] for x in order[:-1]]
    for copy in sent:
        copy.wait_send()


def local(
    query_latent,
    joint_latent,
    rotary_key,
    query_gain,
    joint_gain,
    query_weight,
    query_rotary,
    key_weight,
    value_weight,
    output_weight,
    expert_input,
    expert_gain,
    routes,
    route_weight,
    gate_weight,
    up_weight,
    down_weight,
):
    n = lax.axis_size("ep")
    m = lax.axis_size("tp")
    nz = m // 2
    rows, width = expert_input.shape
    local_count = gate_weight.shape[0]
    capacity = 3 * rows // (2 * n)
    turn = rotary_key.shape[1]
    half_turn = turn // 2
    head_count = key_weight.shape[1] // NOPE
    latent_half = joint_latent.shape[1] // 2
    tokens = n * rows
    batch = local_count * capacity
    block_width = width // m
    row_block = rows // m
    half = width // 2
    dims = (n, m, rows, width, local_count, capacity, head_count, turn)

    powers = (ROTARY_BASE ** (-np.arange(half_turn) / half_turn)).astype(np.float32)
    freq_col = jnp.asarray(powers[:, None])
    freq_row = jnp.asarray(np.tile(powers, 2 * head_count)[None, :])

    small = [
        routes.T,
        route_weight.T,
        rotary_key.T,
        freq_col,
        freq_row,
        query_gain[None, :],
        joint_gain[None, :],
        expert_gain[None, :],
    ]
    large = [
        query_latent,
        joint_latent,
        query_weight,
        query_rotary,
        key_weight,
        value_weight,
        output_weight,
        expert_input,
        gate_weight,
        up_weight,
        down_weight,
    ]

    def like(source):
        return pltpu.VMEM(source.shape, source.dtype)

    def buffer(*shape):
        return pltpu.VMEM(shape, BF16)

    dma = pltpu.SemaphoreType.DMA
    scratch = [
        like(query_latent),
        buffer(2, n, rows, latent_half),
        like(query_weight),
        like(query_rotary),
        like(key_weight),
        like(value_weight),
        like(output_weight),
        like(expert_input),
        like(gate_weight),
        like(up_weight),
        like(down_weight),
        pltpu.VMEM((n, 8, rows), F32),
        buffer(rows, half),
        buffer(n - 1, local_count, capacity, half * SHARED_EIGHTHS // 8),
        buffer(n - 1, local_count, capacity, half - 2 * (half * SHARED_EIGHTHS // 8)),
        buffer(2, local_count, n * capacity, half),
        buffer(n, rows, batch),
        buffer(n, turn, rows),
        buffer(head_count, rows, NOPE + turn),
        buffer(head_count, NOPE + turn, tokens),
        buffer(tokens, head_count * VDIM),
        buffer(rows, head_count * VDIM),
        buffer(m, row_block, width),
        buffer(nz, row_block, width),
        buffer(nz, row_block, width),
        buffer(nz, local_count, n * capacity, block_width),
        buffer(nz, local_count, n * capacity, block_width),
        buffer(nz, local_count, n * capacity, block_width),
        buffer(nz, n, local_count, capacity, block_width),
        buffer(nz - 1, rows, block_width),
        buffer(nz, rows, block_width),
        dma((12,)),
    ]
    line = [(n,), (n,), (2, n), (n,), (n,), (n,), (n,), (3, n), (nz,), (nz,), (3, local_count), (nz, n), (nz,)]
    for shape in line:
        scratch += [dma(shape), dma(shape)]

    vmem = pl.BlockSpec(memory_space=pltpu.VMEM)
    anywhere = pl.BlockSpec(memory_space=pl.ANY)
    return pl.pallas_call(
        functools.partial(kernel, dims),
        in_specs=[vmem] * len(small) + [anywhere] * len(large),
        out_specs=(vmem, vmem),
        out_shape=(
            jax.ShapeDtypeStruct((row_block, width), BF16),
            jax.ShapeDtypeStruct((rows, block_width), BF16),
        ),
        scratch_shapes=scratch,
        compiler_params=pltpu.CompilerParams(
            collective_id=0, has_side_effects=True, vmem_limit_bytes=67043328
        ),
        name="whole",
    )(*small, *large)


def solution(mesh):
    return jax.shard_map(
        local,
        mesh=mesh,
        in_specs=(
            P("ep", None),
            P("ep", None),
            P("ep", None),
            P(),
            P(),
            P(None, "tp"),
            P(None, "tp"),
            P(None, "tp"),
            P(None, "tp"),
            P("tp", None),
            P("ep", None),
            P(),
            P("ep", None),
            P("ep", None),
            P("ep", None, "tp"),
            P("ep", None, "tp"),
            P("ep", "tp", None),
        ),
        out_specs=(P(("ep", "tp"), None), P("ep", "tp")),
        check_vma=False,
    )
```
